256 devices in a mesh: grp: 2 (over y), tp: 16 (over z), dp: 8 (over x, core).
Axes of the slice: x: 4, y: 2, z: 16, core: 2. Of those that a mesh axis runs over, the one named last changes fastest.
The devices are a block of a 4x16x16 slice.
Arguments:
- tokens: bfloat16 [256, 4096], P('grp', 'dp'), parts along dimension 0, may hold values from -50 to 50
- lengths: int32 [256], P(('grp', 'dp')), parts along dimension 0, may hold values from 1 to 24, as said below
- norm_gain: float32 [2, 4096], P(None, 'dp'), may hold values from 0.1 to 1.9
- w_z: bfloat16 [2, 4096, 4096], P(None, 'dp', 'tp'), may hold values from -0.09375 to 0.09375
- w_x: bfloat16 [2, 4096, 4096], P(None, 'dp', 'tp'), may hold values from -0.09375 to 0.09375
- w_b: bfloat16 [2, 4096, 2048], P(None, 'dp', 'tp'), may hold values from -0.09375 to 0.09375
- w_c: bfloat16 [2, 4096, 2048], P(None, 'dp', 'tp'), may hold values from -0.09375 to 0.09375
- w_dt: bfloat16 [2, 4096, 64], P(None, 'dp'), may hold values from -0.09375 to 0.09375
- conv_weight: bfloat16 [2, 4, 8192], P(None, None, 'tp'), may hold values from -3 to 3
- dt_bias: float32 [2, 64], P(None, 'tp'), may hold values from -6 to -1.5
- a_log: float32 [2, 64], P(None, 'tp'), may hold values from 0 to 2.77
- d_skip: float32 [2, 64], P(None, 'tp'), may hold values from 0.1 to 1.9
- out_gain: float32 [2, 4096], P(None, 'tp'), may hold values from 0.1 to 1.9
- w_out: bfloat16 [2, 4096, 4096], P(None, 'tp', 'dp'), may hold values from -0.09375 to 0.09375
- conv_state: bfloat16 [2, 256, 3, 8192], P(None, ('grp', 'dp'), None, 'tp'), parts along dimension 1, may hold values from -6 to 6
- ssm_state: float32 [2, 256, 64, 64, 128], P(None, ('grp', 'dp'), 'tp'), parts along dimension 1, may hold values from -2 to 2
Outputs:
- mixed_out: bfloat16 [256, 4096], P('grp', 'dp'), parts along dimension 0
- conv_new: bfloat16 [2, 256, 3, 8192], P(None, ('grp', 'dp'), None, 'tp'), parts along dimension 1
- ssm_new: float32 [2, 256, 64, 64, 128], P(None, ('grp', 'dp'), 'tp'), parts along dimension 1
The draws below stay inside these ranges and needn't reach their ends.
There are 2 independent parts, one for each index of `grp`. The reference program is written for one: setup_inputs(seed, part) draws one part's arguments, and reference() takes and returns one part's arrays. A program takes and returns all parts, laid end to end along the dimension named above; an argument that names none is the same for every part. Nothing has to cross between parts.
Inputs may be any that keep to these rules, and one draw needn't show every extreme that they name: `lengths`: each part has at least one sequence of length 24.
All inputs are finite; a program needn't handle non-finite values.
Results may differ from the reference program's by a relative error of at most 0.012.
Values may be sent and summed in bfloat16 or wider, within the bound.
No kernel may reach another device: no remote copies, remote signals or barrier semaphores. Data moves between devices by JAX's collectives and lax.ppermute only.
A program may use at most 64 MiB of HBM per device.

```python
import jax
import jax.numpy as jnp
from jax import lax

D = 4096
HEADS = 64
GROUPS = 16
HEAD_DIM = 64
STATE = 128
CONV_W = 4
LAYERS = 2
BATCH = 128
SSD_W = 4096
CONV_DIM = 8192


def draw_tokens(key, part):
    first_key = jax.random.fold_in(key, 11)
    second_key = jax.random.fold_in(key, 12)
    columns = 10.0 ** (jnp.arange(D, dtype=jnp.float32) / D - 0.5)
    rowscale = jnp.exp(jax.random.uniform(first_key, (BATCH,), jnp.float32, -1.1513, 1.1513))
    entries = jnp.clip(jax.random.normal(second_key, (BATCH, D), jnp.float32), -5.0, 5.0)
    return (entries * rowscale[:, None] * columns[None, :]).astype(jnp.bfloat16)


def draw_lengths(key, part):
    short_key = jax.random.fold_in(key, 21)
    pick_key = jax.random.fold_in(key, 22)
    long_key = jax.random.fold_in(key, 23)
    place_key = jax.random.fold_in(key, 24)
    short_len = jax.random.randint(short_key, (BATCH,), 1, 7, dtype=jnp.int32)
    picked = jax.random.randint(pick_key, (BATCH,), 0, 8, dtype=jnp.int32) == 0
    long_len = jax.random.randint(long_key, (BATCH,), 12, 25, dtype=jnp.int32)
    chosen = jnp.where(picked, long_len, short_len)
    place = jax.random.randint(place_key, (), 0, BATCH, dtype=jnp.int32)
    return jnp.where(jnp.arange(BATCH, dtype=jnp.int32) == place, jnp.int32(24), chosen).astype(jnp.int32)


def block_scale(rng, dims, cuts, smallest, top_value):
    def one(dim, blocks):
        heights = jax.random.uniform(jax.random.fold_in(jax.random.fold_in(rng, 6), dim), (blocks,), jnp.float32, smallest / len(cuts), top_value / len(cuts))
        return jnp.repeat(jnp.exp(heights), dims[dim] // blocks).reshape((-1,) + (1,) * (len(dims) - dim - 1))

    factor_of = one(*cuts[0])
    for cut in cuts[1:]:
        factor_of = factor_of * one(*cut)
    return factor_of


def bell_draw(stream_key, shape, spread, limit, cuts=(), kind=jnp.bfloat16):
    drawn = spread * jax.random.normal(stream_key, shape, jnp.float32)
    if cuts:
        drawn = drawn * block_scale(stream_key, shape, cuts, -0.22, 0.18)
    return jnp.clip(drawn, -limit, limit).astype(kind)


def setup_inputs(seed: int = 0, part: int = 0) -> dict:
    arg_keys = jax.random.split(jax.random.key(seed), 17)
    own_keys = jax.random.split(jax.random.fold_in(arg_keys[16], part), 17)
    return {
        "tokens": draw_tokens(jax.random.fold_in(jax.random.fold_in(arg_keys[16], part), 71), part),
        "lengths": draw_lengths(jax.random.fold_in(jax.random.fold_in(arg_keys[16], part), 71), part),
        "norm_gain": jnp.clip(1.0 + 0.18 * jax.random.normal(arg_keys[2], (LAYERS, D), jnp.float32), 0.1, 1.9),
        "w_z": bell_draw(arg_keys[3], (LAYERS, D, SSD_W), D ** -0.5, 0.09375, ((1, 8), (2, 16))),
        "w_x": bell_draw(arg_keys[4], (LAYERS, D, SSD_W), D ** -0.5, 0.09375, ((1, 8), (2, 16))),
        "w_b": bell_draw(arg_keys[5], (LAYERS, D, GROUPS * STATE), D ** -0.5, 0.09375, ((1, 8), (2, 16))),
        "w_c": bell_draw(arg_keys[6], (LAYERS, D, GROUPS * STATE), D ** -0.5, 0.09375, ((1, 8), (2, 16))),
        "w_dt": bell_draw(arg_keys[7], (LAYERS, D, HEADS), D ** -0.5, 0.09375, ((1, 8),)),
        "conv_weight": bell_draw(arg_keys[8], (LAYERS, CONV_W, CONV_DIM), 0.5, 3.0, ((2, 16),)),
        "dt_bias": jnp.clip(-6.0 + 4.5 * jax.random.uniform(arg_keys[9], (LAYERS, HEADS), jnp.float32) ** block_scale(arg_keys[9], (LAYERS, HEADS), ((1, 16),), -0.2, 0.2), -6.0, -1.5),
        "a_log": jnp.clip(2.77 * jax.random.uniform(arg_keys[10], (LAYERS, HEADS), jnp.float32) ** block_scale(arg_keys[10], (LAYERS, HEADS), ((1, 16),), -0.2, 0.2), 0.0, 2.77),
        "d_skip": jnp.clip(1.0 + 0.18 * jax.random.normal(arg_keys[11], (LAYERS, HEADS), jnp.float32), 0.1, 1.9),
        "out_gain": jnp.clip(1.0 + 0.18 * jax.random.normal(arg_keys[12], (LAYERS, SSD_W), jnp.float32), 0.1, 1.9),
        "w_out": bell_draw(arg_keys[13], (LAYERS, SSD_W, D), SSD_W ** -0.5, 0.09375, ((1, 16), (2, 8))),
        "conv_state": bell_draw(own_keys[14], (LAYERS, BATCH, CONV_W - 1, CONV_DIM), 1.0, 6.0, ((1, 8), (3, 16))),
        "ssm_state": bell_draw(own_keys[15], (LAYERS, BATCH, HEADS, HEAD_DIM, STATE), 0.15, 2.0, ((1, 8), (2, 16)), jnp.float32),
    }


EPSILON = 1e-06

def one_block(stream, lengths, gain, w_z, w_x, w_b, w_c, w_dt, taps_weight, dt_bias, a_log, d_skip, out_gain, w_out, conv_past, ssm_past):
    batch_rows = stream.shape[0]
    per_group = HEADS // GROUPS
    width_x = per_group * HEAD_DIM
    wide = stream.astype(jnp.float32)
    inverse = lax.rsqrt(lax.optimization_barrier(jnp.mean(wide * wide, axis=-1)) + EPSILON)[:, None]
    normed = (wide * gain).astype(jnp.bfloat16)
    gating = (jnp.dot(normed, w_z, preferred_element_type=jnp.float32) * inverse).astype(jnp.bfloat16)
    values = (jnp.dot(normed, w_x, preferred_element_type=jnp.float32) * inverse).astype(jnp.bfloat16)
    writes = (jnp.dot(normed, w_b, preferred_element_type=jnp.float32) * inverse).astype(jnp.bfloat16)
    reads = (jnp.dot(normed, w_c, preferred_element_type=jnp.float32) * inverse).astype(jnp.bfloat16)
    step_raw = jnp.dot(normed, w_dt, preferred_element_type=jnp.float32) * inverse
    current = jnp.concatenate([values.reshape(batch_rows, GROUPS, width_x), writes.reshape(batch_rows, GROUPS, STATE), reads.reshape(batch_rows, GROUPS, STATE)], axis=-1).reshape(batch_rows, CONV_DIM)
    offsets = jnp.arange(CONV_W - 1, dtype=jnp.int32)
    alive = lengths[:, None] + offsets[None, :] >= CONV_W
    history = jnp.where(alive[:, :, None], conv_past, jnp.zeros_like(conv_past))
    conv_next = jnp.concatenate([history[:, 1:], current[:, None]], axis=1)
    summed = current.astype(jnp.float32) * taps_weight[CONV_W - 1].astype(jnp.float32)
    for tap_at in range(CONV_W - 1):
        summed = summed + history[:, tap_at].astype(jnp.float32) * taps_weight[tap_at].astype(jnp.float32)
    activated = jax.nn.silu(summed).reshape(batch_rows, GROUPS, width_x + 2 * STATE)
    head_in = activated[:, :, :width_x].reshape(batch_rows, GROUPS, per_group, HEAD_DIM)
    write_keys = activated[:, :, width_x:width_x + STATE]
    read_keys = activated[:, :, width_x + STATE:]
    step = jax.nn.softplus(step_raw + dt_bias).reshape(batch_rows, GROUPS, per_group)
    decay = jnp.exp(-jnp.exp(a_log).reshape(GROUPS, per_group) * step)
    carried = lengths >= 2
    before = ssm_past.reshape(batch_rows, GROUPS, per_group, HEAD_DIM, STATE)
    before = jnp.where(carried[:, None, None, None, None], before, jnp.zeros_like(before))
    state_next = decay[..., None, None] * before + (step[..., None] * head_in)[..., None] * write_keys[:, :, None, None, :]
    readout = jnp.einsum('bghpn,bgn->bghp', state_next, read_keys, precision=lax.Precision.HIGHEST)
    readout = readout + d_skip.reshape(GROUPS, per_group)[..., None] * head_in
    gated = readout.reshape(batch_rows, GROUPS, width_x) * jax.nn.silu(gating.astype(jnp.float32).reshape(batch_rows, GROUPS, width_x))
    gated = gated * lax.rsqrt(lax.optimization_barrier(jnp.mean(gated * gated, axis=-1, keepdims=True)) + EPSILON) * out_gain.reshape(GROUPS, width_x)
    mixed = gated.reshape(batch_rows, SSD_W).astype(jnp.bfloat16)
    stream_next = (wide + jnp.dot(mixed, w_out, preferred_element_type=jnp.float32)).astype(jnp.bfloat16)
    return (stream_next, conv_next, state_next.reshape(batch_rows, HEADS, HEAD_DIM, STATE))

def reference(tokens, lengths, norm_gain, w_z, w_x, w_b, w_c, w_dt, conv_weight, dt_bias, a_log, d_skip, out_gain, w_out, conv_state, ssm_state):
    stream = tokens
    conv_list = []
    ssm_list = []
    for layer_at in range(LAYERS):
        stream, conv_next, state_next = one_block(stream, lengths, norm_gain[layer_at], w_z[layer_at], w_x[layer_at], w_b[layer_at], w_c[layer_at], w_dt[layer_at], conv_weight[layer_at], dt_bias[layer_at], a_log[layer_at], d_skip[layer_at], out_gain[layer_at], w_out[layer_at], conv_state[layer_at], ssm_state[layer_at])
        conv_list.append(conv_next)
        ssm_list.append(state_next)
    return (stream, jnp.stack(conv_list), jnp.stack(ssm_list))
```

```python
import functools

import jax
import jax.numpy as jnp
from jax import lax
from jax.experimental import pallas as pl
from jax.experimental.pallas import tpu as pltpu
from jax.sharding import PartitionSpec as P

D = 4096
HEADS = 64
GROUPS = 16
HEAD_DIM = 64
STATE = 128
CONV_W = 4
EPSILON = 1e-06
LANES = 128
PIECE = 16
BF16 = jnp.bfloat16
F32 = jnp.float32
MIB = 1 << 20

VMEM_SPEC = pl.BlockSpec(memory_space=pltpu.VMEM)
SMEM_SPEC = pl.BlockSpec(memory_space=pltpu.SMEM)


def params(mib):
    return pltpu.CompilerParams(vmem_limit_bytes=int(mib * MIB))


def iota(shape, dim):
    return lax.broadcasted_iota(jnp.int32, shape, dim)


def dot(a, b, dims):
    return lax.dot_general(a, b, (dims, ((), ())), preferred_element_type=F32)


def split(value):
    high = value.astype(BF16)
    return high, (value - high.astype(F32)).astype(BF16)


def gate_kernel(out_ref):
    out_ref[...] = jnp.zeros_like(out_ref)


def long_cost():
    return pl.CostEstimate(flops=20_000_000_000, bytes_accessed=1_000_000, transcendentals=0)


def gate():
    return pl.pallas_call(
        gate_kernel,
        out_shape=jax.ShapeDtypeStruct((8, LANES), F32),
        out_specs=VMEM_SPEC,
        compiler_params=params(1),
        cost_estimate=long_cost(),
        name="gate",
    )()


def swap(value, mask):
    pairs = [(i, i ^ mask) for i in range(lax.axis_size("dp"))]
    return lax.ppermute(value, "dp", pairs)


def chosen_heads(heads, local_heads):
    row, column = iota((LANES, heads), 0), iota((LANES, heads), 1)
    local = row % PIECE
    first = lax.axis_index("tp") * local_heads
    return ((column == first + local) & (local < local_heads) & (row < 2 * PIECE)).astype(BF16)


def in_pieces(extras, squares):
    lane = iota(extras.shape, 1)
    extras = jnp.where(lane % PIECE == PIECE // 2, squares, extras)
    high, low = split(extras)
    return jnp.where(lane < PIECE, high.astype(F32), low.astype(F32)).astype(BF16)


def first_kernel(local_heads, x_ref, gain_ref, wx_ref, wb_ref, wc_ref, wz_ref, wdt_ref, _, out_ref, extras_ref, *packs):
    wide = x_ref[...].astype(F32)
    normed = (wide * gain_ref[0:1, :]).astype(BF16)
    at = 0
    for ref in (wx_ref, wb_ref, wc_ref, wz_ref):
        width = ref.shape[-1]
        out_ref[:, at : at + width] = dot(normed, ref[0], ((1,), (0,))).astype(BF16)
        for layer, pack in enumerate(packs, 1):
            pack[:, at : at + width] = ref[layer]
        at += width
    chosen = chosen_heads(wdt_ref.shape[1], local_heads)
    own = dot(wdt_ref[0], chosen, ((0,), (1,))).astype(BF16)
    extras_ref[:, :LANES] = dot(normed, own, ((1,), (0,)))
    extras_ref[:, LANES:] = jnp.broadcast_to(jnp.sum(wide * wide, axis=-1, keepdims=True), (wide.shape[0], LANES))
    for layer, pack in enumerate(packs, 1):
        pack[:, at : at + LANES] = dot(wdt_ref[layer], chosen, ((0,), (1,))).astype(BF16)


def finish_kernel(part_ref, extras_ref, out_ref):
    out_ref[...] = in_pieces(extras_ref[:, :LANES], extras_ref[:, LANES:])


def project_first(local_heads, stream, norm_gain, w_x, w_b, w_c, w_z, w_dt):
    rows, features = stream.shape
    width = sum(w.shape[2] for w in (w_x, w_b, w_c, w_z)) + LANES
    parts = jax.ShapeDtypeStruct((rows, width), BF16)
    extras = jax.ShapeDtypeStruct((rows, 2 * LANES), F32)
    packs = [jax.ShapeDtypeStruct((features, width), BF16)] * (w_z.shape[0] - 1)
    inputs = [stream, norm_gain, w_x, w_b, w_c, w_z, w_dt, gate()]
    parts_out, extras_out, *packed = pl.pallas_call(
        functools.partial(first_kernel, local_heads),
        out_shape=(parts, extras, *packs),
        in_specs=[VMEM_SPEC] * len(inputs),
        out_specs=[VMEM_SPEC] * (2 + len(packs)),
        compiler_params=params(8),
        name="project_0",
    )(*inputs)
    last = pl.BlockSpec((rows, LANES), lambda i: (0, width // LANES - 1))
    finished = pl.pallas_call(
        finish_kernel,
        grid=(1,),
        out_shape=parts,
        in_specs=[pl.BlockSpec(memory_space=pl.ANY), pl.BlockSpec((rows, 2 * LANES), lambda i: (0, 0))],
        out_specs=last,
        input_output_aliases={0: 0},
        compiler_params=params(4),
        cost_estimate=long_cost(),
        name="finish_0",
    )(parts_out, extras_out)
    return finished, packed


def later_kernel(layer, stream_ref, own_gain_ref, other_gain_ref, own_ref, other_ref, *out_refs):
    rows = stream_ref.shape[0] // 2
    total, squares = 0.0, 0.0
    for k, (gain, weights) in enumerate(((own_gain_ref, own_ref), (other_gain_ref, other_ref))):
        wide = stream_ref[k * rows : (k + 1) * rows, :].astype(F32)
        normed = (wide * gain[layer : layer + 1, :]).astype(BF16)
        total = total + dot(normed, weights[...], ((1,), (0,)))
        squares = squares + jnp.sum(wide * wide, axis=-1, keepdims=True)
    at = total.shape[1] - LANES
    tail = in_pieces(total[:, at:], squares)
    block = rows // len(out_refs)
    for k, ref in enumerate(out_refs):
        ref[:, :at] = total[k * block : (k + 1) * block, :at].astype(BF16)
        ref[:, at:] = tail[k * block : (k + 1) * block]


def project_later(layer, blocks, stream, own_gain, other_gain, own, other):
    rows = stream.shape[0] // 2
    out = jax.ShapeDtypeStruct((rows // blocks, own.shape[1]), BF16)
    return pl.pallas_call(
        functools.partial(later_kernel, layer),
        out_shape=[out] * blocks,
        in_specs=[VMEM_SPEC] * 5,
        out_specs=[VMEM_SPEC] * blocks,
        compiler_params=params(8),
        cost_estimate=long_cost(),
        name=f"project_{layer}",
    )(stream, own_gain, other_gain, own, other)


def mix_kernel(
    layer, given, *refs
):
    parts_refs, rest = refs[:given], refs[given:]
    mix_body(layer, [part for ref in parts_refs for part in ([ref] if len(ref.shape) == 2 else [ref.at[k] for k in range(ref.shape[0])])], *rest)


def mix_body(
    layer, parts, lengths_ref, taps_ref, bias_ref, alog_ref, skip_ref, gain_ref, past_ref, state_ref,
    mixed_ref, scaled_ref, keys_ref, decay_ref, current_ref,
):
    state, past_ref = state_ref.at[layer], past_ref.at[layer]
    seqs = parts[0].shape[0]
    heads, head_dim, width_n = state.shape[1:]
    width_x = heads * head_dim
    conv = width_x + 2 * width_n
    total = sum(part[...].astype(F32) for part in parts)
    extras = total[:, conv + width_x :]
    extras = extras + pltpu.roll(extras, LANES - PIECE, 1)
    inverse = lax.rsqrt(extras[:, PIECE // 2 : PIECE // 2 + 1] / D + EPSILON)
    current = (total[:, :conv] * inverse).astype(BF16)
    gating = (total[:, conv : conv + width_x] * inverse).astype(BF16).astype(F32)
    current_ref[...] = current

    row = iota((seqs, 1), 0)
    lengths = jnp.zeros((seqs, 1), jnp.int32)
    for s in range(seqs):
        lengths = jnp.where(row == s, lengths_ref[s], lengths)
    taps = taps_ref[layer].astype(F32)
    summed = current.astype(F32) * taps[CONV_W - 1 : CONV_W]
    for j in range(CONV_W - 1):
        past = past_ref[j].astype(F32)
        summed = summed + jnp.where(lengths + j >= CONV_W, past, 0.0) * taps[j : j + 1]
    activated = summed / (1.0 + jnp.exp(-summed))
    head_in = activated[:, :width_x]
    write_keys = activated[:, width_x : width_x + width_n]
    read_keys = activated[:, width_x + width_n :]

    raw = extras[:, :heads] * inverse + bias_ref[layer : layer + 1, :]
    step = jnp.maximum(raw, 0.0) + jnp.log1p(jnp.exp(-jnp.abs(raw)))
    decay = jnp.exp(-jnp.exp(alog_ref[layer : layer + 1, :]) * step)
    decay = jnp.where(lengths >= 2, decay, 0.0)
    lane = iota((seqs, width_x), 1)

    def spread(value):
        out = value[:, 0:1]
        for h in range(1, heads):
            out = jnp.where(lane >= h * head_dim, value[:, h : h + 1], out)
        return out

    scaled = spread(step) * head_in
    scaled_ref[...] = scaled
    keys_ref[...] = write_keys
    decay_ref[...] = decay

    high, low = split(read_keys)
    left = jnp.concatenate(
        [jnp.concatenate([high, high], axis=1), jnp.concatenate([low, jnp.zeros_like(low)], axis=1)], axis=0
    )
    seen = jnp.zeros((seqs, width_x), F32)
    for s in range(seqs):
        old_high, old_low = split(state[s].reshape(width_x, width_n))
        both = dot(left, jnp.concatenate([old_high, old_low], axis=1), ((1,), (1,)))
        seen = jnp.where(row == s, both[:seqs] + both[seqs:], seen)
    pair = jnp.sum(write_keys * read_keys, axis=-1, keepdims=True)
    readout = spread(decay) * seen + scaled * pair + spread(skip_ref[layer : layer + 1, :]) * head_in
    gated = readout * (gating / (1.0 + jnp.exp(-gating)))
    mean = jnp.mean(gated * gated, axis=-1, keepdims=True)
    mixed = (gated * lax.rsqrt(mean + EPSILON) * gain_ref[layer : layer + 1, :]).astype(BF16)
    mixed_ref[...] = mixed


def mix(layer, parts, lengths, taps, bias, alog, skip, gain, past, state):
    seqs = parts[0].shape[-2]
    heads, head_dim, width_n = state.shape[2:]
    width_x = heads * head_dim
    shapes = (
        jax.ShapeDtypeStruct((seqs, width_x), BF16),
        jax.ShapeDtypeStruct((seqs, width_x), F32),
        jax.ShapeDtypeStruct((seqs, width_n), F32),
        jax.ShapeDtypeStruct((seqs, heads), F32),
        jax.ShapeDtypeStruct((seqs, width_x + 2 * width_n), BF16),
    )
    return pl.pallas_call(
        functools.partial(mix_kernel, layer, len(parts)),
        out_shape=shapes,
        in_specs=[*[VMEM_SPEC] * len(parts), SMEM_SPEC, *[VMEM_SPEC] * 7],
        out_specs=[VMEM_SPEC] * len(shapes),
        compiler_params=params(12),
        name=f"mix_{layer}",
    )(*parts, lengths, taps, bias, alog, skip, gain, past, state)


def output_kernel(layer, given, *refs):
    mixed = jnp.concatenate([ref[...] for ref in refs[:given]], axis=0)
    own_ref, other_ref, out_ref = refs[given:]
    rows = mixed.shape[0]
    for k, ref in enumerate((own_ref, other_ref)):
        out_ref[k * rows : (k + 1) * rows, :] = dot(mixed, ref[layer], ((1,), (0,))).astype(BF16)


def output(layer, mixed, own, other):
    rows = sum(m.shape[0] for m in mixed)
    return pl.pallas_call(
        functools.partial(output_kernel, layer, len(mixed)),
        out_shape=jax.ShapeDtypeStruct((2 * rows, own.shape[2]), BF16),
        in_specs=[VMEM_SPEC] * (len(mixed) + 2),
        out_specs=VMEM_SPEC,
        compiler_params=params(4),
        name=f"output_{layer}",
    )(*mixed, own, other)


def block_at(k):
    at = lax.axis_index("dp")
    return lax.bitwise_xor(at // 2, jnp.int32(k)) * 2 + at % 2


def add_kernel(block, parts_ref, *refs):
    streams, out_ref = refs[:-1], refs[-1]
    copies, rows, _ = parts_ref.shape
    total = sum(parts_ref[k].astype(F32) for k in range(copies))
    at = lax.axis_index("tp")
    if len(streams) == 1:
        old = streams[0][pl.ds(pl.multiple_of(at * rows, rows), rows), :]
    else:
        half = copies // 2
        group = lax.rem(at, half)
        per = block // rows
        start = block_at(group // per) * block + lax.rem(group, per) * rows
        picked = [ref[pl.ds(pl.multiple_of(start, rows), rows), :] for ref in streams]
        old = jnp.where(at < half, picked[0], picked[1])
    new = (old.astype(F32) + total).astype(BF16)
    if len(out_ref.shape) == 2:
        out_ref[...] = new
    else:
        for k in range(copies):
            out_ref[k] = new


def add(layer, block, last, parts, streams):
    shape = parts.shape[1:] if last else parts.shape
    return pl.pallas_call(
        functools.partial(add_kernel, block),
        out_shape=jax.ShapeDtypeStruct(shape, BF16),
        in_specs=[VMEM_SPEC] * (1 + len(streams)),
        out_specs=VMEM_SPEC,
        compiler_params=params(4),
        name=f"add_{layer}",
    )(parts, *streams)


def spread_kernel(own_ref, other_ref, out_ref):
    copies = out_ref.shape[0]
    value = jnp.where(lax.axis_index("tp") < copies // 2, own_ref[...], other_ref[...])
    for k in range(copies):
        out_ref[k] = value


def spread(copies, own, other):
    return pl.pallas_call(
        spread_kernel,
        out_shape=jax.ShapeDtypeStruct((copies, *own.shape), BF16),
        in_specs=[VMEM_SPEC] * 2,
        out_specs=VMEM_SPEC,
        compiler_params=params(4),
        name="spread",
    )(own, other)


def order_kernel(block, parts_ref, out_ref):
    copies, rows, _ = parts_ref.shape
    per = block // rows
    half = copies // 2
    for k in range(copies // per):
        value = jnp.concatenate([parts_ref[k * per + s] for s in range(per)], axis=0)
        index = block_at(k % (half // per))
        if k >= half // per:
            index = lax.bitwise_xor(index, jnp.int32(1))
        out_ref[pl.ds(pl.multiple_of(index * block, block), block), :] = value


def order(block, parts):
    copies, rows, features = parts.shape
    return pl.pallas_call(
        functools.partial(order_kernel, block),
        out_shape=jax.ShapeDtypeStruct((copies * rows, features), BF16),
        in_specs=[VMEM_SPEC],
        out_specs=VMEM_SPEC,
        compiler_params=params(4),
        name="order",
    )(parts)


def states_kernel(lengths_ref, past_ref, state_ref, *refs):
    layers = len(refs) // 4
    inputs, (conv_ref, new_ref, columns) = refs[: 4 * layers], refs[4 * layers :]
    layer, chunk = pl.program_id(0), pl.program_id(1)
    seqs, heads, head_dim, width_n = state_ref.shape[1:]

    def of_layer(k, pick):
        out = pick(inputs[k])
        for at in range(1, layers):
            out = jnp.where(layer == at, pick(inputs[4 * at + k]), out)
        return out

    @pl.when(chunk == 0)
    def _():
        scaled = of_layer(0, lambda r: r[...])
        rest = jnp.zeros((LANES - scaled.shape[0], scaled.shape[1]), F32)
        columns[...] = jnp.concatenate([scaled, rest], axis=0).T
        all_seqs = past_ref.shape[2]
        row = iota((all_seqs, 1), 0)
        lengths = jnp.zeros((all_seqs, 1), jnp.int32)
        for s in range(all_seqs):
            lengths = jnp.where(row == s, lengths_ref[s], lengths)
        for j in range(1, CONV_W - 1):
            past = past_ref[0, j].astype(F32)
            conv_ref[0, j - 1] = jnp.where(lengths + j >= CONV_W, past, 0.0).astype(BF16)
        conv_ref[0, CONV_W - 2] = of_layer(3, lambda r: r[...])

    mine = pltpu.roll(columns[...], (LANES - chunk * seqs) % LANES, 1)
    for k in range(seqs):
        at = chunk * seqs + k
        keys = of_layer(1, lambda r: r[pl.ds(at, 1), :])
        decay = of_layer(2, lambda r: r[pl.ds(at, 1), :])
        for h in range(heads):
            column = mine[h * head_dim : (h + 1) * head_dim, k : k + 1]
            new_ref[0, k, h] = decay[:, h : h + 1] * state_ref[0, k, h] + column * keys


def states(lengths, past, state, mixes, seqs):
    layers, all_seqs, heads, head_dim, width_n = state.shape
    inputs = [a for one in mixes for a in one]
    state_spec = pl.BlockSpec((1, seqs, heads, head_dim, width_n), lambda l, c: (l, c, 0, 0, 0))
    past_spec = pl.BlockSpec((1, *past.shape[1:]), lambda l, c: (l, 0, 0, 0))
    return pl.pallas_call(
        states_kernel,
        grid=(layers, all_seqs // seqs),
        out_shape=(jax.ShapeDtypeStruct(past.shape, past.dtype), jax.ShapeDtypeStruct(state.shape, F32)),
        in_specs=[
            SMEM_SPEC,
            past_spec,
            state_spec,
            *(pl.BlockSpec(a.shape, lambda l, c: (0, 0)) for a in inputs),
        ],
        out_specs=(past_spec, state_spec),
        scratch_shapes=[pltpu.VMEM((heads * head_dim, LANES), F32)],
        compiler_params=params(8),
        cost_estimate=pl.CostEstimate(flops=40_000_000, bytes_accessed=8 * state.size, transcendentals=0),
        name="states",
    )(lengths, past, state, *inputs)


def exchange(blocks, axis):
    return lax.all_to_all(blocks, axis, 0, 0, tiled=True)


def body(
    tokens, lengths, norm_gain, w_z, w_x, w_b, w_c, w_dt, conv_weight, dt_bias, a_log, d_skip, out_gain, w_out,
    conv_state, ssm_state,
):
    tp, dp = lax.axis_size("tp"), lax.axis_size("dp")
    if GROUPS != tp or dp & (dp - 1):
        raise ValueError("unexpected mesh")
    local_heads = HEADS // tp
    rows, features = tokens.shape
    block = rows // dp
    layers = w_z.shape[0]
    w_dt = jnp.swapaxes(w_dt, 1, 2)
    past = jnp.swapaxes(conv_state, 1, 2)
    across = [2 * k for k in range(1, dp // 2)]
    other_out = swap(w_out, 1)
    parts, own_packs = project_first(local_heads, tokens, norm_gain, w_x, w_b, w_c, w_z, w_dt)
    parts = [exchange(parts.reshape(dp, block, -1), "dp")]
    mixes = []
    for layer in range(layers):
        mixed, *rest = mix(
            layer, parts, lengths, conv_weight, dt_bias, a_log, d_skip, out_gain, past, ssm_state
        )
        mixes.append(rest)
        if layer == 0:
            mixed, given = lax.optimization_barrier((mixed, (tokens, norm_gain, own_packs)))
            given = [swap(a, 1) for a in jax.tree.leaves(given)]
        mixed = [mixed, *(swap(mixed, mask) for mask in across)]
        if layer == 0:
            mixed, (other_tokens, other_gain, *other_packs) = lax.optimization_barrier((mixed, given))
            streams = [tokens, other_tokens]
        share = output(layer, mixed, w_out, other_out)
        share = exchange(share.reshape(tp, rows // tp, features), "tp")
        new = add(layer, block, layer == layers - 1, share, streams)
        if layer == layers - 1:
            new = spread(tp, new, swap(new, 1))
        new = exchange(new, "tp")
        if layer < layers - 1:
            streams = [new.reshape(rows, features)]
            k = layer
            first, *others = project_later(
                layer + 1, dp // 2, streams[0], norm_gain, other_gain, own_packs[k], other_packs[k]
            )
            parts = [first, *(swap(part, mask) for part, mask in zip(others, across))]
    conv_new, ssm_new = states(lengths, past, ssm_state, mixes, 4)
    return order(block, new), jnp.swapaxes(conv_new, 1, 2), ssm_new


def solution(mesh):
    by_seq = ("grp", "dp")
    placed = (
        P("grp", "dp"),
        P(by_seq),
        P(None, "dp"),
        P(None, "dp", "tp"),
        P(None, "dp", "tp"),
        P(None, "dp", "tp"),
        P(None, "dp", "tp"),
        P(None, "dp", None),
        P(None, None, "tp"),
        P(None, "tp"),
        P(None, "tp"),
        P(None, "tp"),
        P(None, "tp"),
        P(None, "tp", "dp"),
        P(None, by_seq, None, "tp"),
        P(None, by_seq, "tp", None, None),
    )
    return jax.shard_map(
        body,
        mesh=mesh,
        in_specs=placed,
        out_specs=(P("grp", "dp"), P(None, by_seq, None, "tp"), P(None, by_seq, "tp", None, None)),
        check_vma=False,
    )
```

```python
import functools

import jax
import jax.numpy as jnp
from jax import lax
from jax.experimental import pallas as pl
from jax.experimental.pallas import tpu as pltpu
from jax.sharding import PartitionSpec as P


D = 4096
HEADS = 64
GROUPS = 16
CONV_W = 4
EPSILON = 1e-06
LANES = 128
PIECE = 16
BF16 = jnp.bfloat16
F32 = jnp.float32
MIB = 1 << 20

VMEM_SPEC = pl.BlockSpec(memory_space=pltpu.VMEM)


def params(mib):
    return pltpu.CompilerParams(vmem_limit_bytes=int(mib * MIB))


def iota(shape, dim):
    return lax.broadcasted_iota(jnp.int32, shape, dim)


def dot(a, b, dims):
    return lax.dot_general(a, b, (dims, ((), ())), preferred_element_type=F32)


def as_column(ref):
    count = ref.shape[1]
    same = iota((count, count), 0) == iota((count, count), 1)
    row = jnp.broadcast_to(ref[...].astype(F32), (count, count))
    return jnp.sum(jnp.where(same, row, 0.0), axis=1, keepdims=True)


def split(value):
    high = value.astype(BF16)
    return high, (value - high.astype(F32)).astype(BF16)


def gate_kernel(out_ref):
    out_ref[...] = jnp.zeros_like(out_ref)


def long_cost():
    return pl.CostEstimate(flops=20_000_000_000, bytes_accessed=1_000_000, transcendentals=0)


def gate():
    return pl.pallas_call(
        gate_kernel,
        out_shape=jax.ShapeDtypeStruct((8, LANES), F32),
        out_specs=VMEM_SPEC,
        compiler_params=params(1),
        cost_estimate=long_cost(),
        name="gate",
    )()


def swap(value, mask):
    pairs = [(i, i ^ mask) for i in range(lax.axis_size("dp"))]
    return lax.ppermute(value, "dp", pairs)


def chosen_heads(heads, local_heads):
    row, column = iota((LANES, heads), 0), iota((LANES, heads), 1)
    local = row % PIECE
    first = lax.axis_index("tp") * local_heads
    return ((column == first + local) & (local < local_heads) & (row < 2 * PIECE)).astype(BF16)


def in_pieces(extras, squares):
    lane = iota(extras.shape, 1)
    extras = jnp.where(lane % PIECE == PIECE // 2, squares, extras)
    high, low = split(extras)
    return jnp.where(lane < PIECE, high.astype(F32), low.astype(F32)).astype(BF16)


def first_kernel(local_heads, x_ref, gain_ref, wx_ref, wb_ref, wc_ref, wz_ref, wdt_ref, _, out_ref, extras_ref, *packs):
    wide = x_ref[...].astype(F32)
    normed = (wide * gain_ref[0:1, :]).astype(BF16)
    at = 0
    for ref in (wx_ref, wb_ref, wc_ref, wz_ref):
        width = ref.shape[-1]
        out_ref[:, at : at + width] = dot(normed, ref[0], ((1,), (0,))).astype(BF16)
        for layer, pack in enumerate(packs, 1):
            pack[:, at : at + width] = ref[layer]
        at += width
    chosen = chosen_heads(wdt_ref.shape[1], local_heads)
    own = dot(wdt_ref[0], chosen, ((0,), (1,))).astype(BF16)
    extras_ref[:, :LANES] = dot(normed, own, ((1,), (0,)))
    extras_ref[:, LANES:] = jnp.broadcast_to(jnp.sum(wide * wide, axis=-1, keepdims=True), (wide.shape[0], LANES))
    for layer, pack in enumerate(packs, 1):
        pack[:, at : at + LANES] = dot(wdt_ref[layer], chosen, ((0,), (1,))).astype(BF16)


def finish_kernel(part_ref, extras_ref, out_ref):
    out_ref[...] = in_pieces(extras_ref[:, :LANES], extras_ref[:, LANES:])


def project_first(local_heads, stream, norm_gain, w_x, w_b, w_c, w_z, w_dt):
    rows, features = stream.shape
    width = sum(w.shape[2] for w in (w_x, w_b, w_c, w_z)) + LANES
    parts = jax.ShapeDtypeStruct((rows, width), BF16)
    extras = jax.ShapeDtypeStruct((rows, 2 * LANES), F32)
    packs = [jax.ShapeDtypeStruct((features, width), BF16)] * (w_z.shape[0] - 1)
    inputs = [stream, norm_gain, w_x, w_b, w_c, w_z, w_dt, gate()]
    parts_out, extras_out, *packed = pl.pallas_call(
        functools.partial(first_kernel, local_heads),
        out_shape=(parts, extras, *packs),
        in_specs=[VMEM_SPEC] * len(inputs),
        out_specs=[VMEM_SPEC] * (2 + len(packs)),
        compiler_params=params(8),
        name="project_0",
    )(*inputs)
    last = pl.BlockSpec((rows, LANES), lambda i: (0, width // LANES - 1))
    finished = pl.pallas_call(
        finish_kernel,
        grid=(1,),
        out_shape=parts,
        in_specs=[pl.BlockSpec(memory_space=pl.ANY), pl.BlockSpec((rows, 2 * LANES), lambda i: (0, 0))],
        out_specs=last,
        input_output_aliases={0: 0},
        compiler_params=params(4),
        cost_estimate=long_cost(),
        name="finish_0",
    )(parts_out, extras_out)
    return finished, packed


def later_kernel(layer, stream_ref, own_gain_ref, other_gain_ref, own_ref, other_ref, *out_refs):
    rows = stream_ref.shape[0] // 2
    total, squares = 0.0, 0.0
    for k, (gain, weights) in enumerate(((own_gain_ref, own_ref), (other_gain_ref, other_ref))):
        wide = stream_ref[k * rows : (k + 1) * rows, :].astype(F32)
        normed = (wide * gain[layer : layer + 1, :]).astype(BF16)
        total = total + dot(normed, weights[...], ((1,), (0,)))
        squares = squares + jnp.sum(wide * wide, axis=-1, keepdims=True)
    at = total.shape[1] - LANES
    tail = in_pieces(total[:, at:], squares)
    block = rows // len(out_refs)
    for k, ref in enumerate(out_refs):
        ref[:, :at] = total[k * block : (k + 1) * block, :at].astype(BF16)
        ref[:, at:] = tail[k * block : (k + 1) * block]


def project_later(layer, blocks, stream, own_gain, other_gain, own, other):
    rows = stream.shape[0] // 2
    out = jax.ShapeDtypeStruct((rows // blocks, own.shape[1]), BF16)
    return pl.pallas_call(
        functools.partial(later_kernel, layer),
        out_shape=[out] * blocks,
        in_specs=[VMEM_SPEC] * 5,
        out_specs=[VMEM_SPEC] * blocks,
        compiler_params=params(8),
        cost_estimate=long_cost(),
    )(stream, own_gain, other_gain, own, other)


def mix_kernel(
    layer, given, *refs
):
    parts_refs, rest = refs[:given], refs[given:]
    mix_body(layer, [part for ref in parts_refs for part in ([ref] if len(ref.shape) == 2 else [ref.at[k] for k in range(ref.shape[0])])], *rest)


def mix_body(
    layer, parts, lengths_ref, taps_ref, bias_ref, alog_ref, skip_ref, gain_ref, past_ref, state_ref,
    mixed_ref, scaled_ref, keys_ref, decay_ref, current_ref,
):
    state, past_ref = state_ref.at[layer], past_ref.at[layer]
    seqs = parts[0].shape[0]
    heads, head_dim, width_n = state.shape[1:]
    width_x = heads * head_dim
    conv = width_x + 2 * width_n
    total = sum(part[...].astype(F32) for part in parts)
    extras = total[:, conv + width_x :]
    extras = extras + pltpu.roll(extras, LANES - PIECE, 1)
    inverse = lax.rsqrt(extras[:, PIECE // 2 : PIECE // 2 + 1] / D + EPSILON)
    current = (total[:, :conv] * inverse).astype(BF16)
    gating = (total[:, conv : conv + width_x] * inverse).astype(BF16).astype(F32)
    current_ref[...] = current

    row = iota((seqs, 1), 0)
    lengths = as_column(lengths_ref)
    taps = taps_ref[layer].astype(F32)
    summed = current.astype(F32) * taps[CONV_W - 1 : CONV_W]
    for j in range(CONV_W - 1):
        past = past_ref[j].astype(F32)
        summed = summed + jnp.where(lengths + j >= CONV_W, past, 0.0) * taps[j : j + 1]
    activated = summed / (1.0 + jnp.exp(-summed))
    head_in = activated[:, :width_x]
    write_keys = activated[:, width_x : width_x + width_n]
    read_keys = activated[:, width_x + width_n :]

    raw = extras[:, :heads] * inverse + bias_ref[layer : layer + 1, :]
    step = jnp.maximum(raw, 0.0) + jnp.log1p(jnp.exp(-jnp.abs(raw)))
    decay = jnp.exp(-jnp.exp(alog_ref[layer : layer + 1, :]) * step)
    decay = jnp.where(lengths >= 2, decay, 0.0)
    lane = iota((seqs, width_x), 1)

    def spread(value):
        out = value[:, 0:1]
        for h in range(1, heads):
            out = jnp.where(lane >= h * head_dim, value[:, h : h + 1], out)
        return out

    scaled = spread(step) * head_in
    scaled_ref[...] = scaled
    keys_ref[...] = write_keys
    decay_ref[...] = decay

    high, low = split(read_keys)
    left = jnp.concatenate(
        [jnp.concatenate([high, high], axis=1), jnp.concatenate([low, jnp.zeros_like(low)], axis=1)], axis=0
    )
    seen = jnp.zeros((seqs, width_x), F32)
    for s in range(seqs):
        old_high, old_low = split(state[s].reshape(width_x, width_n))
        both = dot(left, jnp.concatenate([old_high, old_low], axis=1), ((1,), (1,)))
        seen = jnp.where(row == s, both[:seqs] + both[seqs:], seen)
    pair = jnp.sum(write_keys * read_keys, axis=-1, keepdims=True)
    readout = spread(decay) * seen + scaled * pair + spread(skip_ref[layer : layer + 1, :]) * head_in
    gated = readout * (gating / (1.0 + jnp.exp(-gating)))
    mean = jnp.mean(gated * gated, axis=-1, keepdims=True)
    mixed = (gated * lax.rsqrt(mean + EPSILON) * gain_ref[layer : layer + 1, :]).astype(BF16)
    mixed_ref[...] = mixed


def mix(layer, parts, lengths, taps, bias, alog, skip, gain, past, state):
    seqs = parts[0].shape[-2]
    heads, head_dim, width_n = state.shape[2:]
    width_x = heads * head_dim
    shapes = (
        jax.ShapeDtypeStruct((seqs, width_x), BF16),
        jax.ShapeDtypeStruct((seqs, width_x), F32),
        jax.ShapeDtypeStruct((seqs, width_n), F32),
        jax.ShapeDtypeStruct((seqs, heads), F32),
        jax.ShapeDtypeStruct((seqs, width_x + 2 * width_n), BF16),
    )
    return pl.pallas_call(
        functools.partial(mix_kernel, layer, len(parts)),
        out_shape=shapes,
        in_specs=[*[VMEM_SPEC] * (len(parts) + 8)],
        out_specs=[VMEM_SPEC] * len(shapes),
        compiler_params=params(12),
    )(*parts, lengths, taps, bias, alog, skip, gain, past, state)


def output_kernel(layer, given, *refs):
    mixed = jnp.concatenate([ref[...] for ref in refs[:given]], axis=0)
    own_ref, other_ref, out_ref = refs[given:]
    rows = mixed.shape[0]
    for k, ref in enumerate((own_ref, other_ref)):
        out_ref[k * rows : (k + 1) * rows, :] = dot(mixed, ref[layer], ((1,), (0,))).astype(BF16)


def output(layer, mixed, own, other):
    rows = sum(m.shape[0] for m in mixed)
    return pl.pallas_call(
        functools.partial(output_kernel, layer, len(mixed)),
        out_shape=jax.ShapeDtypeStruct((2 * rows, own.shape[2]), BF16),
        in_specs=[VMEM_SPEC] * (len(mixed) + 2),
        out_specs=VMEM_SPEC,
        compiler_params=params(4),
    )(*mixed, own, other)


def block_at(k):
    at = lax.axis_index("dp")
    return lax.bitwise_xor(at // 2, jnp.int32(k)) * 2 + at % 2


def add_kernel(block, parts_ref, *refs):
    streams, out_ref = refs[:-1], refs[-1]
    copies, rows, _ = parts_ref.shape
    total = sum(parts_ref[k].astype(F32) for k in range(copies))
    at = lax.axis_index("tp")
    if len(streams) == 1:
        old = streams[0][pl.ds(pl.multiple_of(at * rows, rows), rows), :]
    else:
        half = copies // 2
        group = lax.rem(at, half)
        per = block // rows
        start = block_at(group // per) * block + lax.rem(group, per) * rows
        picked = [ref[pl.ds(pl.multiple_of(start, rows), rows), :] for ref in streams]
        old = jnp.where(at < half, picked[0], picked[1])
    new = (old.astype(F32) + total).astype(BF16)
    if len(out_ref.shape) == 2:
        out_ref[...] = new
    else:
        for k in range(copies):
            out_ref[k] = new


def add(block, last, parts, streams):
    shape = parts.shape[1:] if last else parts.shape
    return pl.pallas_call(
        functools.partial(add_kernel, block),
        out_shape=jax.ShapeDtypeStruct(shape, BF16),
        in_specs=[VMEM_SPEC] * (1 + len(streams)),
        out_specs=VMEM_SPEC,
        compiler_params=params(4),
    )(parts, *streams)


def spread_kernel(own_ref, other_ref, out_ref):
    copies = out_ref.shape[0]
    value = jnp.where(lax.axis_index("tp") < copies // 2, own_ref[...], other_ref[...])
    for k in range(copies):
        out_ref[k] = value


def spread(copies, own, other):
    return pl.pallas_call(
        spread_kernel,
        out_shape=jax.ShapeDtypeStruct((copies, *own.shape), BF16),
        in_specs=[VMEM_SPEC] * 2,
        out_specs=VMEM_SPEC,
        compiler_params=params(4),
        name="spread",
    )(own, other)


def order_kernel(block, parts_ref, out_ref):
    copies, rows, _ = parts_ref.shape
    per = block // rows
    half = copies // 2
    for k in range(copies // per):
        value = jnp.concatenate([parts_ref[k * per + s] for s in range(per)], axis=0)
        index = block_at(k % (half // per))
        if k >= half // per:
            index = lax.bitwise_xor(index, jnp.int32(1))
        out_ref[pl.ds(pl.multiple_of(index * block, block), block), :] = value


def order(block, parts):
    copies, rows, features = parts.shape
    return pl.pallas_call(
        functools.partial(order_kernel, block),
        out_shape=jax.ShapeDtypeStruct((copies * rows, features), BF16),
        in_specs=[VMEM_SPEC],
        out_specs=VMEM_SPEC,
        compiler_params=params(4),
        name="order",
    )(parts)


def states_kernel(lengths_ref, past_ref, state_ref, *refs):
    layers = len(refs) // 4
    inputs, (conv_ref, new_ref, columns) = refs[: 4 * layers], refs[4 * layers :]
    layer, chunk = pl.program_id(0), pl.program_id(1)
    seqs, heads, head_dim, _ = state_ref.shape[1:]

    def of_layer(k, pick):
        out = pick(inputs[k])
        for at in range(1, layers):
            out = jnp.where(layer == at, pick(inputs[4 * at + k]), out)
        return out

    @pl.when(chunk == 0)
    def _():
        scaled = of_layer(0, lambda r: r[...])
        rest = jnp.zeros((LANES - scaled.shape[0], scaled.shape[1]), F32)
        columns[...] = jnp.concatenate([scaled, rest], axis=0).T
        lengths = as_column(lengths_ref)
        for j in range(1, CONV_W - 1):
            past = past_ref[0, j].astype(F32)
            conv_ref[0, j - 1] = jnp.where(lengths + j >= CONV_W, past, 0.0).astype(BF16)
        conv_ref[0, CONV_W - 2] = of_layer(3, lambda r: r[...])

    mine = pltpu.roll(columns[...], (LANES - chunk * seqs) % LANES, 1)
    for k in range(seqs):
        at = chunk * seqs + k
        keys = of_layer(1, lambda r: r[pl.ds(at, 1), :])
        decay = of_layer(2, lambda r: r[pl.ds(at, 1), :])
        for h in range(heads):
            column = mine[h * head_dim : (h + 1) * head_dim, k : k + 1]
            new_ref[0, k, h] = decay[:, h : h + 1] * state_ref[0, k, h] + column * keys


def states(lengths, past, state, mixes, seqs):
    layers, all_seqs, heads, head_dim, width_n = state.shape
    inputs = [a for one in mixes for a in one]
    state_spec = pl.BlockSpec((1, seqs, heads, head_dim, width_n), lambda l, c: (l, c, 0, 0, 0))
    past_spec = pl.BlockSpec((1, *past.shape[1:]), lambda l, c: (l, 0, 0, 0))
    return pl.pallas_call(
        states_kernel,
        grid=(layers, all_seqs // seqs),
        out_shape=(jax.ShapeDtypeStruct(past.shape, past.dtype), jax.ShapeDtypeStruct(state.shape, F32)),
        in_specs=[
            pl.BlockSpec(lengths.shape, lambda l, c: (0, 0)),
            past_spec,
            state_spec,
            *(pl.BlockSpec(a.shape, lambda l, c: (0, 0)) for a in inputs),
        ],
        out_specs=(past_spec, state_spec),
        scratch_shapes=[pltpu.VMEM((heads * head_dim, LANES), F32)],
        compiler_params=params(8),
        cost_estimate=pl.CostEstimate(flops=40_000_000, bytes_accessed=8 * state.size, transcendentals=0),
        name="states",
    )(lengths, past, state, *inputs)


def exchange(blocks, axis):
    return lax.all_to_all(blocks, axis, 0, 0, tiled=True)


def body(
    tokens, lengths, norm_gain, w_z, w_x, w_b, w_c, w_dt, conv_weight, dt_bias, a_log, d_skip, out_gain, w_out,
    conv_state, ssm_state,
):
    tp, dp = lax.axis_size("tp"), lax.axis_size("dp")
    if GROUPS != tp or dp & (dp - 1):
        raise ValueError("unexpected mesh")
    local_heads = HEADS // tp
    rows, features = tokens.shape
    block = rows // dp
    layers = w_z.shape[0]
    w_dt = jnp.swapaxes(w_dt, 1, 2)
    past = jnp.swapaxes(conv_state, 1, 2)
    lengths = lengths.reshape(1, -1)
    across = [2 * k for k in range(1, dp // 2)]
    parts, own_packs = project_first(local_heads, tokens, norm_gain, w_x, w_b, w_c, w_z, w_dt)
    parts = [exchange(parts.reshape(dp, block, -1), "dp")]
    mixes = []
    for layer in range(layers):
        mixed, *rest = mix(
            layer, parts, lengths, conv_weight, dt_bias, a_log, d_skip, out_gain, past, ssm_state
        )
        mixes.append(rest)
        if layer == 0:
            mixed, given = lax.optimization_barrier((mixed, (w_out, tokens, norm_gain, own_packs)))
            given = [swap(a, 1) for a in jax.tree.leaves(given)]
        mixed = [mixed, *(swap(mixed, mask) for mask in across)]
        if layer == 0:
            mixed, (other_out, other_tokens, other_gain, *other_packs) = lax.optimization_barrier((mixed, given))
            streams = [tokens, other_tokens]
        share = output(layer, mixed, w_out, other_out)
        share = exchange(share.reshape(tp, rows // tp, features), "tp")
        new = add(block, layer == layers - 1, share, streams)
        if layer == layers - 1:
            new = spread(tp, new, swap(new, 1))
        new = exchange(new, "tp")
        if layer < layers - 1:
            streams = [new.reshape(rows, features)]
            k = layer
            first, *others = project_later(
                layer + 1, dp // 2, streams[0], norm_gain, other_gain, own_packs[k], other_packs[k]
            )
            parts = [first, *(swap(part, mask) for part, mask in zip(others, across))]
    conv_new, ssm_new = states(lengths, past, ssm_state, mixes, 4)
    return order(block, new), jnp.swapaxes(conv_new, 1, 2), ssm_new


def solution(mesh):
    by_seq = ("grp", "dp")
    placed = (
        P("grp", "dp"),
        P(by_seq),
        P(None, "dp"),
        P(None, "dp", "tp"),
        P(None, "dp", "tp"),
        P(None, "dp", "tp"),
        P(None, "dp", "tp"),
        P(None, "dp", None),
        P(None, None, "tp"),
        P(None, "tp"),
        P(None, "tp"),
        P(None, "tp"),
        P(None, "tp"),
        P(None, "tp", "dp"),
        P(None, by_seq, None, "tp"),
        P(None, by_seq, "tp", None, None),
    )
    return jax.shard_map(
        body,
        mesh=mesh,
        in_specs=placed,
        out_specs=(P("grp", "dp"), P(None, by_seq, None, "tp"), P(None, by_seq, "tp", None, None)),
        check_vma=False,
    )
```

```python
import functools

import jax
import jax.numpy as jnp
from jax import lax
from jax.experimental import pallas as pl
from jax.experimental.pallas import tpu as pltpu
from jax.sharding import PartitionSpec as P

D = 4096
HEADS = 64
GROUPS = 16
HEAD_DIM = 64
STATE = 128
CONV_W = 4
EPSILON = 1e-06
LANES = 128
PIECE = 16
PIECES = 4
BF16 = jnp.bfloat16
F32 = jnp.float32
MIB = 1 << 20

VMEM_SPEC = pl.BlockSpec(memory_space=pltpu.VMEM)


def params(mib):
    return pltpu.CompilerParams(vmem_limit_bytes=int(mib * MIB))


def iota(shape, dim):
    return lax.broadcasted_iota(jnp.int32, shape, dim)


def dot(a, b, dims):
    return lax.dot_general(a, b, (dims, ((), ())), preferred_element_type=F32)


def as_column(ref):
    count = ref.shape[1]
    same = iota((count, count), 0) == iota((count, count), 1)
    row = jnp.broadcast_to(ref[...].astype(F32), (count, count))
    return jnp.sum(jnp.where(same, row, 0.0), axis=1, keepdims=True)


def split(value):
    high = value.astype(BF16)
    return high, (value - high.astype(F32)).astype(BF16)


def gate_kernel(out_ref):
    out_ref[...] = jnp.zeros_like(out_ref)


def long_cost():
    return pl.CostEstimate(flops=20_000_000_000, bytes_accessed=1_000_000, transcendentals=0)


def gate():
    return pl.pallas_call(
        gate_kernel,
        out_shape=jax.ShapeDtypeStruct((8, LANES), F32),
        out_specs=VMEM_SPEC,
        compiler_params=params(1),
        cost_estimate=long_cost(),
        name="gate",
    )()


def swap(value, mask):
    pairs = [(i, i ^ mask) for i in range(lax.axis_size("dp"))]
    return lax.ppermute(value, "dp", pairs)


def chosen_heads(heads, local_heads):
    row, column = iota((LANES, heads), 0), iota((LANES, heads), 1)
    local = row % PIECE
    first = lax.axis_index("tp") * local_heads
    return ((column == first + local) & (local < local_heads) & (row < 2 * PIECE)).astype(BF16)


def in_pieces(extras, squares):
    lane = iota(extras.shape, 1)
    extras = jnp.where(lane % PIECE == PIECE // 2, squares, extras)
    high, low = split(extras)
    return jnp.where(lane < PIECE, high.astype(F32), low.astype(F32)).astype(BF16)


def first_kernel(local_heads, x_ref, gain_ref, wx_ref, wb_ref, wc_ref, wz_ref, wdt_ref, _, out_ref, extras_ref, *packs):
    wide = x_ref[...].astype(F32)
    normed = (wide * gain_ref[0:1, :]).astype(BF16)
    at = 0
    for ref in (wx_ref, wb_ref, wc_ref, wz_ref):
        width = ref.shape[-1]
        out_ref[:, at : at + width] = dot(normed, ref[0], ((1,), (0,))).astype(BF16)
        for layer, pack in enumerate(packs, 1):
            pack[: wide.shape[1], at : at + width] = ref[layer]
        at += width
    chosen = chosen_heads(wdt_ref.shape[1], local_heads)
    own = dot(wdt_ref[0], chosen, ((0,), (1,))).astype(BF16)
    extras_ref[:, :LANES] = dot(normed, own, ((1,), (0,)))
    extras_ref[:, LANES:] = jnp.broadcast_to(jnp.sum(wide * wide, axis=-1, keepdims=True), (wide.shape[0], LANES))
    features = wide.shape[1]
    for layer, pack in enumerate(packs, 1):
        pack[:features, at : at + LANES] = dot(wdt_ref[layer], chosen, ((0,), (1,))).astype(BF16)
        row = iota((PIECE, features), 0)
        left = jnp.broadcast_to(gain_ref[layer : layer + 1, :], row.shape)
        gains = jnp.zeros_like(left)
        for k in range(3):
            piece = left.astype(BF16).astype(F32)
            gains = jnp.where(row == k, piece, gains)
            left = left - piece
        pack[features : features + PIECE, :features] = gains.astype(BF16)
        pack[features + PIECE :, :features] = x_ref[...]


def finish_kernel(part_ref, extras_ref, out_ref):
    out_ref[...] = in_pieces(extras_ref[:, :LANES], extras_ref[:, LANES:])


def project_first(local_heads, stream, norm_gain, w_x, w_b, w_c, w_z, w_dt):
    rows, features = stream.shape
    width = sum(w.shape[2] for w in (w_x, w_b, w_c, w_z)) + LANES
    parts = jax.ShapeDtypeStruct((rows, width), BF16)
    extras = jax.ShapeDtypeStruct((rows, 2 * LANES), F32)
    packs = [jax.ShapeDtypeStruct((features + PIECE + rows, width), BF16)] * (w_z.shape[0] - 1)
    inputs = [stream, norm_gain, w_x, w_b, w_c, w_z, w_dt, gate()]
    parts_out, extras_out, *packed = pl.pallas_call(
        functools.partial(first_kernel, local_heads),
        out_shape=(parts, extras, *packs),
        in_specs=[VMEM_SPEC] * len(inputs),
        out_specs=[VMEM_SPEC] * (2 + len(packs)),
        compiler_params=params(8),
        name="project_0",
    )(*inputs)
    last = pl.BlockSpec((rows, LANES), lambda i: (0, width // LANES - 1))
    finished = pl.pallas_call(
        finish_kernel,
        grid=(1,),
        out_shape=parts,
        in_specs=[pl.BlockSpec(memory_space=pl.ANY), pl.BlockSpec((rows, 2 * LANES), lambda i: (0, 0))],
        out_specs=last,
        input_output_aliases={0: 0},
        compiler_params=params(4),
        cost_estimate=long_cost(),
        name="finish_0",
    )(parts_out, extras_out)
    return finished, packed


def later_kernel(stream_ref, own_ref, other_ref, *out_refs):
    rows, features = stream_ref.shape[0] // 2, stream_ref.shape[1]
    total, squares = 0.0, 0.0
    for k, ref in enumerate((own_ref, other_ref)):
        wide = stream_ref[k * rows : (k + 1) * rows, :].astype(F32)
        pieces = ref[features : features + PIECE, :features].astype(F32)
        gain = pieces[0:1] + pieces[1:2] + pieces[2:3]
        normed = (wide * gain).astype(BF16)
        total = total + dot(normed, ref[:features, :], ((1,), (0,)))
        squares = squares + jnp.sum(wide * wide, axis=-1, keepdims=True)
    at = total.shape[1] - LANES
    tail = in_pieces(total[:, at:], squares)
    block = rows // len(out_refs)
    for k, ref in enumerate(out_refs):
        ref[:, :at] = total[k * block : (k + 1) * block, :at].astype(BF16)
        ref[:, at:] = tail[k * block : (k + 1) * block]


def project_later(layer, blocks, stream, own, other):
    rows = stream.shape[0] // 2
    out = jax.ShapeDtypeStruct((rows // blocks, own.shape[1]), BF16)
    return pl.pallas_call(
        later_kernel,
        out_shape=[out] * blocks,
        in_specs=[VMEM_SPEC] * 3,
        out_specs=[VMEM_SPEC] * blocks,
        compiler_params=params(8),
        cost_estimate=long_cost(),
        name=f"project_{layer}",
    )(stream, own, other)


def mix_kernel(
    layer, given, *refs
):
    parts_refs, rest = refs[:given], refs[given:]
    mix_body(layer, [part for ref in parts_refs for part in ([ref] if len(ref.shape) == 2 else [ref.at[k] for k in range(ref.shape[0])])], *rest)


def mix_body(
    layer, parts, lengths_ref, taps_ref, bias_ref, alog_ref, skip_ref, gain_ref, past_ref, state_ref,
    mixed_ref, scaled_ref, keys_ref, decay_ref, current_ref,
):
    state, past_ref = state_ref.at[layer], past_ref.at[layer]
    seqs = parts[0].shape[0]
    heads, head_dim, width_n = state.shape[1:]
    width_x = heads * head_dim
    conv = width_x + 2 * width_n
    total = sum(part[...].astype(F32) for part in parts)
    extras = total[:, conv + width_x :]
    extras = extras + pltpu.roll(extras, LANES - PIECE, 1)
    inverse = lax.rsqrt(extras[:, PIECE // 2 : PIECE // 2 + 1] / D + EPSILON)
    current = (total[:, :conv] * inverse).astype(BF16)
    gating = (total[:, conv : conv + width_x] * inverse).astype(BF16).astype(F32)
    current_ref[...] = current

    row = iota((seqs, 1), 0)
    lengths = as_column(lengths_ref)
    taps = taps_ref[layer].astype(F32)
    summed = current.astype(F32) * taps[CONV_W - 1 : CONV_W]
    for j in range(CONV_W - 1):
        past = past_ref[j].astype(F32)
        summed = summed + jnp.where(lengths + j >= CONV_W, past, 0.0) * taps[j : j + 1]
    activated = summed / (1.0 + jnp.exp(-summed))
    head_in = activated[:, :width_x]
    write_keys = activated[:, width_x : width_x + width_n]
    read_keys = activated[:, width_x + width_n :]

    raw = extras[:, :heads] * inverse + bias_ref[layer : layer + 1, :]
    step = jnp.maximum(raw, 0.0) + jnp.log1p(jnp.exp(-jnp.abs(raw)))
    decay = jnp.exp(-jnp.exp(alog_ref[layer : layer + 1, :]) * step)
    decay = jnp.where(lengths >= 2, decay, 0.0)
    lane = iota((seqs, width_x), 1)

    def spread(value):
        out = value[:, 0:1]
        for h in range(1, heads):
            out = jnp.where(lane >= h * head_dim, value[:, h : h + 1], out)
        return out

    scaled = spread(step) * head_in
    scaled_ref[...] = scaled
    keys_ref[...] = write_keys
    decay_ref[...] = decay

    high, low = split(read_keys)
    left = jnp.concatenate(
        [jnp.concatenate([high, high], axis=1), jnp.concatenate([low, jnp.zeros_like(low)], axis=1)], axis=0
    )
    seen = jnp.zeros((seqs, width_x), F32)
    for s in range(seqs):
        old_high, old_low = split(state[s].reshape(width_x, width_n))
        both = dot(left, jnp.concatenate([old_high, old_low], axis=1), ((1,), (1,)))
        seen = jnp.where(row == s, both[:seqs] + both[seqs:], seen)
    pair = jnp.sum(write_keys * read_keys, axis=-1, keepdims=True)
    readout = spread(decay) * seen + scaled * pair + spread(skip_ref[layer : layer + 1, :]) * head_in
    gated = readout * (gating / (1.0 + jnp.exp(-gating)))
    mean = jnp.mean(gated * gated, axis=-1, keepdims=True)
    mixed = (gated * lax.rsqrt(mean + EPSILON) * gain_ref[layer : layer + 1, :]).astype(BF16)
    mixed_ref[...] = mixed


def mix(layer, parts, lengths, taps, bias, alog, skip, gain, past, state):
    seqs = parts[0].shape[-2]
    heads, head_dim, width_n = state.shape[2:]
    width_x = heads * head_dim
    shapes = (
        jax.ShapeDtypeStruct((seqs, width_x), BF16),
        jax.ShapeDtypeStruct((seqs, width_x), F32),
        jax.ShapeDtypeStruct((seqs, width_n), F32),
        jax.ShapeDtypeStruct((seqs, heads), F32),
        jax.ShapeDtypeStruct((seqs, width_x + 2 * width_n), BF16),
    )
    return pl.pallas_call(
        functools.partial(mix_kernel, layer, len(parts)),
        out_shape=shapes,
        in_specs=[*[VMEM_SPEC] * (len(parts) + 8)],
        out_specs=[VMEM_SPEC] * len(shapes),
        compiler_params=params(12),
        name=f"mix_{layer}",
    )(*parts, lengths, taps, bias, alog, skip, gain, past, state)


def output_kernel(layer, given, *refs):
    mixed = jnp.concatenate([ref[...] for ref in refs[:given]], axis=0)
    own_ref, other_ref, out_ref = refs[given:]
    rows = mixed.shape[0]
    for k, ref in enumerate((own_ref, other_ref)):
        out_ref[k * rows : (k + 1) * rows, :] = dot(mixed, ref[layer], ((1,), (0,))).astype(BF16)


def output(layer, mixed, own, other):
    rows = sum(m.shape[0] for m in mixed)
    return pl.pallas_call(
        functools.partial(output_kernel, layer, len(mixed)),
        out_shape=jax.ShapeDtypeStruct((2 * rows, own.shape[2]), BF16),
        in_specs=[VMEM_SPEC] * (len(mixed) + 2),
        out_specs=VMEM_SPEC,
        compiler_params=params(4),
        name=f"output_{layer}",
    )(*mixed, own, other)


def block_at(k):
    at = lax.axis_index("dp")
    return lax.bitwise_xor(at // 2, jnp.int32(k)) * 2 + at % 2


def add_kernel(block, parts_ref, *refs):
    streams, out_ref = refs[:-1], refs[-1]
    copies, rows, _ = parts_ref.shape
    total = sum(parts_ref[k].astype(F32) for k in range(copies))
    at = lax.axis_index("tp")
    if len(streams) == 1:
        old = streams[0][pl.ds(pl.multiple_of(at * rows, rows), rows), :]
    else:
        half = copies // 2
        group = lax.rem(at, half)
        per = block // rows
        start = block_at(group // per) * block + lax.rem(group, per) * rows
        first, second = streams
        features = out_ref.shape[-1]
        lowest = second.shape[0] - first.shape[0]
        picked = [
            first[pl.ds(pl.multiple_of(start, rows), rows), :],
            second[pl.ds(pl.multiple_of(lowest + start, rows), rows), :features],
        ]
        old = jnp.where(at < half, picked[0], picked[1])
    new = (old.astype(F32) + total).astype(BF16)
    if len(out_ref.shape) == 2:
        out_ref[...] = new
    else:
        for k in range(copies):
            out_ref[k] = new


def add(layer, block, last, parts, streams):
    shape = parts.shape[1:] if last else parts.shape
    return pl.pallas_call(
        functools.partial(add_kernel, block),
        out_shape=jax.ShapeDtypeStruct(shape, BF16),
        in_specs=[VMEM_SPEC] * (1 + len(streams)),
        out_specs=VMEM_SPEC,
        compiler_params=params(4),
        name=f"add_{layer}",
    )(parts, *streams)


def spread_kernel(own_ref, other_ref, out_ref):
    copies = out_ref.shape[0]
    value = jnp.where(lax.axis_index("tp") < copies // 2, own_ref[...], other_ref[...])
    for k in range(copies):
        out_ref[k] = value


def spread(copies, own, other):
    return pl.pallas_call(
        spread_kernel,
        out_shape=jax.ShapeDtypeStruct((copies, *own.shape), BF16),
        in_specs=[VMEM_SPEC] * 2,
        out_specs=VMEM_SPEC,
        compiler_params=params(4),
        name="spread",
    )(own, other)


def order_kernel(block, parts_ref, out_ref):
    copies, rows, _ = parts_ref.shape
    per = block // rows
    half = copies // 2
    for k in range(copies // per):
        value = jnp.concatenate([parts_ref[k * per + s] for s in range(per)], axis=0)
        index = block_at(k % (half // per))
        if k >= half // per:
            index = lax.bitwise_xor(index, jnp.int32(1))
        out_ref[pl.ds(pl.multiple_of(index * block, block), block), :] = value


def order(block, parts):
    copies, rows, features = parts.shape
    return pl.pallas_call(
        functools.partial(order_kernel, block),
        out_shape=jax.ShapeDtypeStruct((copies * rows, features), BF16),
        in_specs=[VMEM_SPEC],
        out_specs=VMEM_SPEC,
        compiler_params=params(4),
        name="order",
    )(parts)


def states_kernel(layer, pieces, lengths_ref, past_ref, state_ref, scaled_ref, keys_ref, decay_ref, current_ref, *refs):
    conv_ref, new_ref, columns, conv, new, left = refs[-6:]
    seqs, heads, head_dim, width_n = new.shape
    piece = seqs // pieces

    def copy(k):
        rows = pl.ds(k * piece, piece)
        return pltpu.make_async_copy(new.at[rows], new_ref.at[layer, rows], left.at[k])

    scaled = scaled_ref[...]
    rest = jnp.zeros((LANES - seqs, scaled.shape[1]), F32)
    columns[...] = jnp.concatenate([scaled, rest], axis=0).T
    for s in range(seqs):
        for h in range(heads):
            column = columns[h * head_dim : (h + 1) * head_dim, s : s + 1]
            old = decay_ref[s : s + 1, h : h + 1] * state_ref[layer, s, h]
            new[s, h] = old + column * keys_ref[s : s + 1, :]
        if s % piece == 0 and s > 0:
            copy(s // piece - 1).start()
    lengths = as_column(lengths_ref)
    for j in range(1, CONV_W - 1):
        past = past_ref[layer, j].astype(F32)
        conv[j - 1] = jnp.where(lengths + j >= CONV_W, past, 0.0).astype(BF16)
    conv[CONV_W - 2] = current_ref[...]
    copy(pieces - 1).start()
    for k in range(pieces):
        copy(k).wait()
    last = pltpu.make_async_copy(conv, conv_ref.at[layer], left.at[pieces])
    last.start()
    last.wait()


def states(layer, pieces, lengths, past, state, scaled, keys, decay, current, before):
    seqs, heads, head_dim, width_n = state.shape[1:]
    anywhere = pl.BlockSpec(memory_space=pl.ANY)
    inputs = (lengths, past, state, scaled, keys, decay, current)
    return pl.pallas_call(
        functools.partial(states_kernel, layer, pieces),
        out_shape=(jax.ShapeDtypeStruct(past.shape, past.dtype), jax.ShapeDtypeStruct(state.shape, F32)),
        in_specs=[*[VMEM_SPEC] * len(inputs), *[anywhere] * len(before)],
        out_specs=(anywhere, anywhere),
        input_output_aliases={len(inputs) + k: k for k in range(len(before))},
        scratch_shapes=[
            pltpu.VMEM((heads * head_dim, LANES), F32),
            pltpu.VMEM(past.shape[1:], BF16),
            pltpu.VMEM(state.shape[1:], F32),
            pltpu.SemaphoreType.DMA((pieces + 1,)),
        ],
        compiler_params=params(8),
        cost_estimate=pl.CostEstimate(flops=2_000_000_000, bytes_accessed=4 * state.size, transcendentals=0),
        name=f"states_{layer}",
    )(*inputs, *before)


def exchange(blocks, axis):
    return lax.all_to_all(blocks, axis, 0, 0, tiled=True)


def body(
    tokens, lengths, norm_gain, w_z, w_x, w_b, w_c, w_dt, conv_weight, dt_bias, a_log, d_skip, out_gain, w_out,
    conv_state, ssm_state,
):
    tp, dp = lax.axis_size("tp"), lax.axis_size("dp")
    if GROUPS != tp or dp & (dp - 1):
        raise ValueError("unexpected mesh")
    local_heads = HEADS // tp
    rows, features = tokens.shape
    block = rows // dp
    layers = w_z.shape[0]
    w_dt = jnp.swapaxes(w_dt, 1, 2)
    past = jnp.swapaxes(conv_state, 1, 2)
    lengths = lengths.reshape(1, -1)
    across = [2 * k for k in range(1, dp // 2)]
    parts, own_packs = project_first(local_heads, tokens, norm_gain, w_x, w_b, w_c, w_z, w_dt)
    other_packs = [swap(pack, 1) for pack in own_packs]
    parts = [exchange(parts.reshape(dp, block, -1), "dp")]
    other_out = swap(w_out, 1)
    streams = [tokens, other_packs[0]]
    made = ()
    for layer in range(layers):
        last = layer == layers - 1
        mixed, *rest = mix(
            layer, parts, lengths, conv_weight, dt_bias, a_log, d_skip, out_gain, past, ssm_state
        )
        mixed = [mixed, *(swap(mixed, mask) for mask in across)]
        if layer == 0:
            mixed, other_packs = lax.optimization_barrier((mixed, other_packs))
        if last:
            made = states(layer, PIECES, lengths, past, ssm_state, *rest, made)
            mixed, made = lax.optimization_barrier((mixed, made))
        share = output(layer, mixed, w_out, other_out)
        share = exchange(share.reshape(tp, rows // tp, features), "tp")
        new = add(layer, block, last, share, streams)
        if last:
            new = spread(tp, new, swap(new, 1))
        new = exchange(new, "tp")
        if not last:
            streams = [new.reshape(rows, features)]
            parts = project_later(
                layer + 1, dp // 2, streams[0], own_packs[layer], other_packs[layer]
            )
            parts, rest = lax.optimization_barrier((parts, rest))
            first, *others = parts
            parts = [first, *(swap(part, mask) for part, mask in zip(others, across))]
            made = states(layer, PIECES, lengths, past, ssm_state, *rest, made)
            parts, made = lax.optimization_barrier((parts, made))
    conv_new, ssm_new = made
    return order(block, new), jnp.swapaxes(conv_new, 1, 2), ssm_new


def solution(mesh):
    by_seq = ("grp", "dp")
    placed = (
        P("grp", "dp"),
        P(by_seq),
        P(None, "dp"),
        P(None, "dp", "tp"),
        P(None, "dp", "tp"),
        P(None, "dp", "tp"),
        P(None, "dp", "tp"),
        P(None, "dp", None),
        P(None, None, "tp"),
        P(None, "tp"),
        P(None, "tp"),
        P(None, "tp"),
        P(None, "tp"),
        P(None, "tp", "dp"),
        P(None, by_seq, None, "tp"),
        P(None, by_seq, "tp", None, None),
    )
    return jax.shard_map(
        body,
        mesh=mesh,
        in_specs=placed,
        out_specs=(P("grp", "dp"), P(None, by_seq, None, "tp"), P(None, by_seq, "tp", None, None)),
        check_vma=False,
    )
```

```python
import functools

import jax
import jax.numpy as jnp
from jax import lax
from jax.experimental import pallas as pl
from jax.experimental.pallas import tpu as pltpu
from jax.sharding import PartitionSpec as P

D = 4096
HEADS = 64
GROUPS = 16
HEAD_DIM = 64
STATE = 128
CONV_W = 4
EPSILON = 1e-06
LANES = 128
PIECE = 16
PIECES = 4
BF16 = jnp.bfloat16
F32 = jnp.float32
MIB = 1 << 20

VMEM_SPEC = pl.BlockSpec(memory_space=pltpu.VMEM)


def params(mib):
    return pltpu.CompilerParams(vmem_limit_bytes=int(mib * MIB))


def iota(shape, dim):
    return lax.broadcasted_iota(jnp.int32, shape, dim)


def dot(a, b, dims):
    return lax.dot_general(a, b, (dims, ((), ())), preferred_element_type=F32)


def as_column(ref):
    count = ref.shape[1]
    same = iota((count, count), 0) == iota((count, count), 1)
    row = jnp.broadcast_to(ref[...].astype(F32), (count, count))
    return jnp.sum(jnp.where(same, row, 0.0), axis=1, keepdims=True)


def split(value):
    high = value.astype(BF16)
    return high, (value - high.astype(F32)).astype(BF16)


def gate_kernel(out_ref):
    out_ref[...] = jnp.zeros_like(out_ref)


def long_cost():
    return pl.CostEstimate(flops=20_000_000_000, bytes_accessed=1_000_000, transcendentals=0)


def gate():
    return pl.pallas_call(
        gate_kernel,
        out_shape=jax.ShapeDtypeStruct((8, LANES), F32),
        out_specs=VMEM_SPEC,
        compiler_params=params(1),
        cost_estimate=long_cost(),
        name="gate",
    )()


def swap(value, mask):
    pairs = [(i, i ^ mask) for i in range(lax.axis_size("dp"))]
    return lax.ppermute(value, "dp", pairs)


def chosen_heads(heads, local_heads):
    row, column = iota((LANES, heads), 0), iota((LANES, heads), 1)
    local = row % PIECE
    first = lax.axis_index("tp") * local_heads
    return ((column == first + local) & (local < local_heads) & (row < 2 * PIECE)).astype(BF16)


def in_pieces(extras, squares):
    lane = iota(extras.shape, 1)
    extras = jnp.where(lane % PIECE == PIECE // 2, squares, extras)
    high, low = split(extras)
    return jnp.where(lane < PIECE, high.astype(F32), low.astype(F32)).astype(BF16)


def first_kernel(local_heads, x_ref, gain_ref, wx_ref, wb_ref, wc_ref, wz_ref, wdt_ref, _, out_ref, extras_ref, *packs):
    wide = x_ref[...].astype(F32)
    normed = (wide * gain_ref[0:1, :]).astype(BF16)
    at = 0
    for ref in (wx_ref, wb_ref, wc_ref, wz_ref):
        width = ref.shape[-1]
        out_ref[:, at : at + width] = dot(normed, ref[0], ((1,), (0,))).astype(BF16)
        for layer, pack in enumerate(packs, 1):
            pack[: wide.shape[1], at : at + width] = ref[layer]
        at += width
    chosen = chosen_heads(wdt_ref.shape[1], local_heads)
    own = dot(wdt_ref[0], chosen, ((0,), (1,))).astype(BF16)
    extras_ref[:, :LANES] = dot(normed, own, ((1,), (0,)))
    extras_ref[:, LANES:] = jnp.broadcast_to(jnp.sum(wide * wide, axis=-1, keepdims=True), (wide.shape[0], LANES))
    features = wide.shape[1]
    for layer, pack in enumerate(packs, 1):
        pack[:features, at : at + LANES] = dot(wdt_ref[layer], chosen, ((0,), (1,))).astype(BF16)
        row = iota((PIECE, features), 0)
        left = jnp.broadcast_to(gain_ref[layer : layer + 1, :], row.shape)
        gains = jnp.zeros_like(left)
        for k in range(3):
            piece = left.astype(BF16).astype(F32)
            gains = jnp.where(row == k, piece, gains)
            left = left - piece
        pack[features : features + PIECE, :features] = gains.astype(BF16)
        pack[features + PIECE :, :features] = x_ref[...]


def finish_kernel(part_ref, extras_ref, out_ref):
    out_ref[...] = in_pieces(extras_ref[:, :LANES], extras_ref[:, LANES:])


def project_first(local_heads, stream, norm_gain, w_x, w_b, w_c, w_z, w_dt):
    rows, features = stream.shape
    width = sum(w.shape[2] for w in (w_x, w_b, w_c, w_z)) + LANES
    parts = jax.ShapeDtypeStruct((rows, width), BF16)
    extras = jax.ShapeDtypeStruct((rows, 2 * LANES), F32)
    packs = [jax.ShapeDtypeStruct((features + PIECE + rows, width), BF16)] * (w_z.shape[0] - 1)
    inputs = [stream, norm_gain, w_x, w_b, w_c, w_z, w_dt, gate()]
    parts_out, extras_out, *packed = pl.pallas_call(
        functools.partial(first_kernel, local_heads),
        out_shape=(parts, extras, *packs),
        in_specs=[VMEM_SPEC] * len(inputs),
        out_specs=[VMEM_SPEC] * (2 + len(packs)),
        compiler_params=params(8),
        name="project_0",
    )(*inputs)
    last = pl.BlockSpec((rows, LANES), lambda i: (0, width // LANES - 1))
    finished = pl.pallas_call(
        finish_kernel,
        grid=(1,),
        out_shape=parts,
        in_specs=[pl.BlockSpec(memory_space=pl.ANY), pl.BlockSpec((rows, 2 * LANES), lambda i: (0, 0))],
        out_specs=last,
        input_output_aliases={0: 0},
        compiler_params=params(4),
        cost_estimate=long_cost(),
        name="finish_0",
    )(parts_out, extras_out)
    return finished, packed


def later_kernel(stream_ref, own_ref, other_ref, *out_refs):
    rows, features = stream_ref.shape[0] // 2, stream_ref.shape[1]
    total, squares = 0.0, 0.0
    for k, ref in enumerate((own_ref, other_ref)):
        wide = stream_ref[k * rows : (k + 1) * rows, :].astype(F32)
        pieces = ref[features : features + PIECE, :features].astype(F32)
        gain = pieces[0:1] + pieces[1:2] + pieces[2:3]
        normed = (wide * gain).astype(BF16)
        total = total + dot(normed, ref[:features, :], ((1,), (0,)))
        squares = squares + jnp.sum(wide * wide, axis=-1, keepdims=True)
    at = total.shape[1] - LANES
    tail = in_pieces(total[:, at:], squares)
    block = rows // len(out_refs)
    for k, ref in enumerate(out_refs):
        ref[:, :at] = total[k * block : (k + 1) * block, :at].astype(BF16)
        ref[:, at:] = tail[k * block : (k + 1) * block]


def project_later(layer, blocks, stream, own, other):
    rows = stream.shape[0] // 2
    out = jax.ShapeDtypeStruct((rows // blocks, own.shape[1]), BF16)
    return pl.pallas_call(
        later_kernel,
        out_shape=[out] * blocks,
        in_specs=[VMEM_SPEC] * 3,
        out_specs=[VMEM_SPEC] * blocks,
        compiler_params=params(8),
        cost_estimate=long_cost(),
        name=f"project_{layer}",
    )(stream, own, other)


def mix_kernel(
    layer, given, *refs
):
    parts_refs, rest = refs[:given], refs[given:]
    mix_body(layer, [part for ref in parts_refs for part in ([ref] if len(ref.shape) == 2 else [ref.at[k] for k in range(ref.shape[0])])], *rest)


def mix_body(
    layer, parts, lengths_ref, taps_ref, bias_ref, alog_ref, skip_ref, gain_ref, past_ref, state_ref,
    mixed_ref, scaled_ref, keys_ref, decay_ref, current_ref,
):
    state, past_ref = state_ref.at[layer], past_ref.at[layer]
    seqs = parts[0].shape[0]
    heads, head_dim, width_n = state.shape[1:]
    width_x = heads * head_dim
    conv = width_x + 2 * width_n
    total = sum(part[...].astype(F32) for part in parts)
    extras = total[:, conv + width_x :]
    extras = extras + pltpu.roll(extras, LANES - PIECE, 1)
    inverse = lax.rsqrt(extras[:, PIECE // 2 : PIECE // 2 + 1] / D + EPSILON)
    current = (total[:, :conv] * inverse).astype(BF16)
    gating = (total[:, conv : conv + width_x] * inverse).astype(BF16).astype(F32)
    current_ref[...] = current

    row = iota((seqs, 1), 0)
    lengths = as_column(lengths_ref)
    taps = taps_ref[layer].astype(F32)
    summed = current.astype(F32) * taps[CONV_W - 1 : CONV_W]
    for j in range(CONV_W - 1):
        past = past_ref[j].astype(F32)
        summed = summed + jnp.where(lengths + j >= CONV_W, past, 0.0) * taps[j : j + 1]
    activated = summed / (1.0 + jnp.exp(-summed))
    head_in = activated[:, :width_x]
    write_keys = activated[:, width_x : width_x + width_n]
    read_keys = activated[:, width_x + width_n :]

    raw = extras[:, :heads] * inverse + bias_ref[layer : layer + 1, :]
    step = jnp.maximum(raw, 0.0) + jnp.log1p(jnp.exp(-jnp.abs(raw)))
    decay = jnp.exp(-jnp.exp(alog_ref[layer : layer + 1, :]) * step)
    decay = jnp.where(lengths >= 2, decay, 0.0)
    lane = iota((seqs, width_x), 1)

    def spread(value):
        out = value[:, 0:1]
        for h in range(1, heads):
            out = jnp.where(lane >= h * head_dim, value[:, h : h + 1], out)
        return out

    scaled = spread(step) * head_in
    scaled_ref[...] = scaled
    keys_ref[...] = write_keys
    decay_ref[...] = decay

    high, low = split(read_keys)
    left = jnp.concatenate(
        [jnp.concatenate([high, high], axis=1), jnp.concatenate([low, jnp.zeros_like(low)], axis=1)], axis=0
    )
    seen = jnp.zeros((seqs, width_x), F32)
    for s in range(seqs):
        old_high, old_low = split(state[s].reshape(width_x, width_n))
        both = dot(left, jnp.concatenate([old_high, old_low], axis=1), ((1,), (1,)))
        seen = jnp.where(row == s, both[:seqs] + both[seqs:], seen)
    pair = jnp.sum(write_keys * read_keys, axis=-1, keepdims=True)
    readout = spread(decay) * seen + scaled * pair + spread(skip_ref[layer : layer + 1, :]) * head_in
    gated = readout * (gating / (1.0 + jnp.exp(-gating)))
    mean = jnp.mean(gated * gated, axis=-1, keepdims=True)
    mixed = (gated * lax.rsqrt(mean + EPSILON) * gain_ref[layer : layer + 1, :]).astype(BF16)
    mixed_ref[...] = mixed


def mix(layer, parts, lengths, taps, bias, alog, skip, gain, past, state):
    seqs = parts[0].shape[-2]
    heads, head_dim, width_n = state.shape[2:]
    width_x = heads * head_dim
    shapes = (
        jax.ShapeDtypeStruct((seqs, width_x), BF16),
        jax.ShapeDtypeStruct((seqs, width_x), F32),
        jax.ShapeDtypeStruct((seqs, width_n), F32),
        jax.ShapeDtypeStruct((seqs, heads), F32),
        jax.ShapeDtypeStruct((seqs, width_x + 2 * width_n), BF16),
    )
    return pl.pallas_call(
        functools.partial(mix_kernel, layer, len(parts)),
        out_shape=shapes,
        in_specs=[*[VMEM_SPEC] * (len(parts) + 8)],
        out_specs=[VMEM_SPEC] * len(shapes),
        compiler_params=params(12),
        name=f"mix_{layer}",
    )(*parts, lengths, taps, bias, alog, skip, gain, past, state)


def output_kernel(layer, given, *refs):
    mixed = jnp.concatenate([ref[...] for ref in refs[:given]], axis=0)
    own_ref, other_ref, out_ref = refs[given:]
    rows = mixed.shape[0]
    for k, ref in enumerate((own_ref, other_ref)):
        out_ref[k * rows : (k + 1) * rows, :] = dot(mixed, ref[layer], ((1,), (0,))).astype(BF16)


def output(layer, mixed, own, other):
    rows = sum(m.shape[0] for m in mixed)
    return pl.pallas_call(
        functools.partial(output_kernel, layer, len(mixed)),
        out_shape=jax.ShapeDtypeStruct((2 * rows, own.shape[2]), BF16),
        in_specs=[VMEM_SPEC] * (len(mixed) + 2),
        out_specs=VMEM_SPEC,
        compiler_params=params(4),
        name=f"output_{layer}",
    )(*mixed, own, other)


def block_at(k):
    at = lax.axis_index("dp")
    return lax.bitwise_xor(at // 2, jnp.int32(k)) * 2 + at % 2


def add_kernel(block, parts_ref, *refs):
    streams, out_ref = refs[:-1], refs[-1]
    copies, rows, _ = parts_ref.shape
    total = sum(parts_ref[k].astype(F32) for k in range(copies))
    at = lax.axis_index("tp")
    if len(streams) == 1:
        old = streams[0][pl.ds(pl.multiple_of(at * rows, rows), rows), :]
    else:
        half = copies // 2
        group = lax.rem(at, half)
        per = block // rows
        start = block_at(group // per) * block + lax.rem(group, per) * rows
        first, second = streams
        features = out_ref.shape[-1]
        lowest = second.shape[0] - first.shape[0]
        picked = [
            first[pl.ds(pl.multiple_of(start, rows), rows), :],
            second[pl.ds(pl.multiple_of(lowest + start, rows), rows), :features],
        ]
        old = jnp.where(at < half, picked[0], picked[1])
    new = (old.astype(F32) + total).astype(BF16)
    for k in range(copies):
        out_ref[k] = new


def add(layer, block, parts, streams):
    return pl.pallas_call(
        functools.partial(add_kernel, block),
        out_shape=jax.ShapeDtypeStruct(parts.shape, BF16),
        in_specs=[VMEM_SPEC] * (1 + len(streams)),
        out_specs=VMEM_SPEC,
        compiler_params=params(4),
        name=f"add_{layer}",
    )(parts, *streams)


def order_kernel(block, own_ref, other_ref, out_ref):
    copies, rows, _ = own_ref.shape
    per = block // rows
    half = copies // 2
    for k in range(half // per):
        index = block_at(k)
        for ref, first, at in ((own_ref, 0, index), (other_ref, half, lax.bitwise_xor(index, jnp.int32(1)))):
            value = jnp.concatenate([ref[first + k * per + s] for s in range(per)], axis=0)
            out_ref[pl.ds(pl.multiple_of(at * block, block), block), :] = value


def order(block, own, other):
    copies, rows, features = own.shape
    return pl.pallas_call(
        functools.partial(order_kernel, block),
        out_shape=jax.ShapeDtypeStruct((copies * rows, features), BF16),
        in_specs=[VMEM_SPEC] * 2,
        out_specs=VMEM_SPEC,
        compiler_params=params(4),
        name="order",
    )(own, other)


def states_kernel(layer, pieces, lengths_ref, past_ref, state_ref, scaled_ref, keys_ref, decay_ref, current_ref, *refs):
    conv_ref, new_ref, columns, conv, new, left = refs[-6:]
    seqs, heads, head_dim, width_n = new.shape
    piece = seqs // pieces

    def copy(k):
        rows = pl.ds(k * piece, piece)
        return pltpu.make_async_copy(new.at[rows], new_ref.at[layer, rows], left.at[k])

    scaled = scaled_ref[...]
    rest = jnp.zeros((LANES - seqs, scaled.shape[1]), F32)
    columns[...] = jnp.concatenate([scaled, rest], axis=0).T
    for s in range(seqs):
        for h in range(heads):
            column = columns[h * head_dim : (h + 1) * head_dim, s : s + 1]
            old = decay_ref[s : s + 1, h : h + 1] * state_ref[layer, s, h]
            new[s, h] = old + column * keys_ref[s : s + 1, :]
        if s % piece == 0 and s > 0:
            copy(s // piece - 1).start()
    lengths = as_column(lengths_ref)
    for j in range(1, CONV_W - 1):
        past = past_ref[layer, j].astype(F32)
        conv[j - 1] = jnp.where(lengths + j >= CONV_W, past, 0.0).astype(BF16)
    conv[CONV_W - 2] = current_ref[...]
    copy(pieces - 1).start()
    for k in range(pieces):
        copy(k).wait()
    last = pltpu.make_async_copy(conv, conv_ref.at[layer], left.at[pieces])
    last.start()
    last.wait()


def states(layer, pieces, lengths, past, state, scaled, keys, decay, current, before):
    seqs, heads, head_dim, width_n = state.shape[1:]
    anywhere = pl.BlockSpec(memory_space=pl.ANY)
    inputs = (lengths, past, state, scaled, keys, decay, current)
    return pl.pallas_call(
        functools.partial(states_kernel, layer, pieces),
        out_shape=(jax.ShapeDtypeStruct(past.shape, past.dtype), jax.ShapeDtypeStruct(state.shape, F32)),
        in_specs=[*[VMEM_SPEC] * len(inputs), *[anywhere] * len(before)],
        out_specs=(anywhere, anywhere),
        input_output_aliases={len(inputs) + k: k for k in range(len(before))},
        scratch_shapes=[
            pltpu.VMEM((heads * head_dim, LANES), F32),
            pltpu.VMEM(past.shape[1:], BF16),
            pltpu.VMEM(state.shape[1:], F32),
            pltpu.SemaphoreType.DMA((pieces + 1,)),
        ],
        compiler_params=params(8),
        cost_estimate=pl.CostEstimate(flops=2_000_000_000, bytes_accessed=4 * state.size, transcendentals=0),
        name=f"states_{layer}",
    )(*inputs, *before)


def exchange(blocks, axis):
    return lax.all_to_all(blocks, axis, 0, 0, tiled=True)


def body(
    tokens, lengths, norm_gain, w_z, w_x, w_b, w_c, w_dt, conv_weight, dt_bias, a_log, d_skip, out_gain, w_out,
    conv_state, ssm_state,
):
    tp, dp = lax.axis_size("tp"), lax.axis_size("dp")
    if GROUPS != tp or dp & (dp - 1):
        raise ValueError("unexpected mesh")
    local_heads = HEADS // tp
    rows, features = tokens.shape
    block = rows // dp
    layers = w_z.shape[0]
    w_dt = jnp.swapaxes(w_dt, 1, 2)
    past = jnp.swapaxes(conv_state, 1, 2)
    lengths = lengths.reshape(1, -1)
    across = [2 * k for k in range(1, dp // 2)]
    parts, own_packs = project_first(local_heads, tokens, norm_gain, w_x, w_b, w_c, w_z, w_dt)
    other_packs = [swap(pack, 1) for pack in own_packs]
    parts = [exchange(parts.reshape(dp, block, -1), "dp")]
    other_out = swap(w_out, 1)
    streams = [tokens, other_packs[0]]
    made = ()
    for layer in range(layers):
        last = layer == layers - 1
        mixed, *rest = mix(
            layer, parts, lengths, conv_weight, dt_bias, a_log, d_skip, out_gain, past, ssm_state
        )
        mixed = [mixed, *(swap(mixed, mask) for mask in across)]
        if layer == 0:
            mixed, other_packs = lax.optimization_barrier((mixed, other_packs))
        if last:
            made = states(layer, PIECES, lengths, past, ssm_state, *rest, made)
            mixed, made = lax.optimization_barrier((mixed, made))
        share = output(layer, mixed, w_out, other_out)
        share = exchange(share.reshape(tp, rows // tp, features), "tp")
        new = exchange(add(layer, block, share, streams), "tp")
        if not last:
            streams = [new.reshape(rows, features)]
            parts = project_later(
                layer + 1, dp // 2, streams[0], own_packs[layer], other_packs[layer]
            )
            parts, rest = lax.optimization_barrier((parts, rest))
            first, *others = parts
            parts = [first, *(swap(part, mask) for part, mask in zip(others, across))]
            made = states(layer, PIECES, lengths, past, ssm_state, *rest, made)
            parts, made = lax.optimization_barrier((parts, made))
    conv_new, ssm_new = made
    return order(block, new, swap(new, 1)), jnp.swapaxes(conv_new, 1, 2), ssm_new


def solution(mesh):
    by_seq = ("grp", "dp")
    placed = (
        P("grp", "dp"),
        P(by_seq),
        P(None, "dp"),
        P(None, "dp", "tp"),
        P(None, "dp", "tp"),
        P(None, "dp", "tp"),
        P(None, "dp", "tp"),
        P(None, "dp", None),
        P(None, None, "tp"),
        P(None, "tp"),
        P(None, "tp"),
        P(None, "tp"),
        P(None, "tp"),
        P(None, "tp", "dp"),
        P(None, by_seq, None, "tp"),
        P(None, by_seq, "tp", None, None),
    )
    return jax.shard_map(
        body,
        mesh=mesh,
        in_specs=placed,
        out_specs=(P("grp", "dp"), P(None, by_seq, None, "tp"), P(None, by_seq, "tp", None, None)),
        check_vma=False,
    )
```

```python
import functools

import jax
import jax.numpy as jnp
from jax import lax
from jax.experimental import pallas as pl
from jax.experimental.pallas import tpu as pltpu
from jax.sharding import PartitionSpec as P

D = 4096
HEADS = 64
GROUPS = 16
HEAD_DIM = 64
STATE = 128
CONV_W = 4
EPSILON = 1e-06
LANES = 128
PIECE = 16
PIECES = 4
BF16 = jnp.bfloat16
F32 = jnp.float32
MIB = 1 << 20

VMEM_SPEC = pl.BlockSpec(memory_space=pltpu.VMEM)


def params(mib):
    return pltpu.CompilerParams(vmem_limit_bytes=int(mib * MIB))


def iota(shape, dim):
    return lax.broadcasted_iota(jnp.int32, shape, dim)


def dot(a, b, dims):
    return lax.dot_general(a, b, (dims, ((), ())), preferred_element_type=F32)


def as_column(ref):
    count = ref.shape[1]
    same = iota((count, count), 0) == iota((count, count), 1)
    row = jnp.broadcast_to(ref[...].astype(F32), (count, count))
    return jnp.sum(jnp.where(same, row, 0.0), axis=1, keepdims=True)


def split(value):
    high = value.astype(BF16)
    return high, (value - high.astype(F32)).astype(BF16)


def gate_kernel(out_ref):
    out_ref[...] = jnp.zeros_like(out_ref)


def long_cost():
    return pl.CostEstimate(flops=20_000_000_000, bytes_accessed=1_000_000, transcendentals=0)


def gate():
    return pl.pallas_call(
        gate_kernel,
        out_shape=jax.ShapeDtypeStruct((8, LANES), F32),
        out_specs=VMEM_SPEC,
        compiler_params=params(1),
        cost_estimate=long_cost(),
        name="gate",
    )()


def swap(value, mask):
    pairs = [(i, i ^ mask) for i in range(lax.axis_size("dp"))]
    return lax.ppermute(value, "dp", pairs)


def chosen_heads(heads, local_heads):
    row, column = iota((LANES, heads), 0), iota((LANES, heads), 1)
    local = row % PIECE
    first = lax.axis_index("tp") * local_heads
    return ((column == first + local) & (local < local_heads) & (row < 2 * PIECE)).astype(BF16)


def with_squares(extras, squares):
    return jnp.where(iota(extras.shape, 1) % PIECE == PIECE // 2, squares, extras)


def in_pieces(extras):
    high, low = split(extras)
    return jnp.where(iota(extras.shape, 1) < PIECE, high.astype(F32), low.astype(F32)).astype(BF16)


def block_at(k):
    at = lax.axis_index("dp")
    return lax.bitwise_xor(at // 2, jnp.int32(k)) * 2 + at % 2


def first_kernel(local_heads, block, x_ref, gain_ref, wx_ref, wb_ref, wc_ref, wz_ref, wdt_ref, _, own_ref, other_ref, *packs):
    rows, features = x_ref.shape
    blocks = [block_at(k) for k in range(rows // block // 2)]
    blocks += [lax.bitwise_xor(b, jnp.int32(1)) for b in blocks]
    tokens = [x_ref[pl.ds(pl.multiple_of(b * block, block), block), :] for b in blocks]
    wide = jnp.concatenate(tokens, axis=0).astype(F32)
    normed = (wide * gain_ref[0:1, :]).astype(BF16)
    half = rows // 2
    at = 0
    for ref in (wx_ref, wb_ref, wc_ref, wz_ref):
        width = ref.shape[-1]
        part = dot(normed, ref[0], ((1,), (0,)))
        own_ref[:, at : at + width] = part[:half]
        other_ref[:, at : at + width] = part[half:].astype(BF16)
        at += width
    chosen = chosen_heads(wdt_ref.shape[1], local_heads)
    steps = dot(wdt_ref[0], chosen, ((0,), (1,))).astype(BF16)
    squares = jnp.sum(wide * wide, axis=-1, keepdims=True)
    extras = with_squares(dot(normed, steps, ((1,), (0,))), squares)
    own_ref[:, at:] = extras[:half]
    other_ref[:, at:] = in_pieces(extras[half:])
    for layer, pack in enumerate(packs, 1):
        first = 0
        for ref in (wx_ref, wb_ref, wc_ref, wz_ref):
            pack[:features, first : first + ref.shape[-1]] = ref[layer]
            first += ref.shape[-1]
        pack[:features, at:] = dot(wdt_ref[layer], chosen, ((0,), (1,))).astype(BF16)
        row = iota((PIECE, features), 0)
        left = jnp.broadcast_to(gain_ref[layer : layer + 1, :], row.shape)
        gains = jnp.zeros_like(left)
        for k in range(3):
            piece = left.astype(BF16).astype(F32)
            gains = jnp.where(row == k, piece, gains)
            left = left - piece
        pack[features : features + PIECE, :features] = gains.astype(BF16)
        pack[features + PIECE :, :features] = x_ref[...]


def combine_kernel(own_ref, arrived_ref, *out_refs):
    total = own_ref[...] + arrived_ref[...].astype(F32)
    at = total.shape[1] - LANES
    pieces = arrived_ref[:, at:].astype(F32)
    whole = pieces + pltpu.roll(pieces, LANES - PIECE, 1)
    whole = jnp.where(iota(whole.shape, 1) < PIECE, whole, pltpu.roll(whole, PIECE, 1))
    tail = in_pieces(own_ref[:, at:] + whole)
    block = total.shape[0] // len(out_refs)
    for k, ref in enumerate(out_refs):
        ref[:, :at] = total[k * block : (k + 1) * block, :at].astype(BF16)
        ref[:, at:] = tail[k * block : (k + 1) * block]


def project_first(local_heads, block, blocks, stream, norm_gain, w_x, w_b, w_c, w_z, w_dt):
    rows, features = stream.shape
    width = sum(w.shape[2] for w in (w_x, w_b, w_c, w_z)) + LANES
    own = jax.ShapeDtypeStruct((rows // 2, width), F32)
    other = jax.ShapeDtypeStruct((rows // 2, width), BF16)
    packs = [jax.ShapeDtypeStruct((features + PIECE + rows, width), BF16)] * (w_z.shape[0] - 1)
    inputs = [stream, norm_gain, w_x, w_b, w_c, w_z, w_dt, gate()]
    own, other, *packed = pl.pallas_call(
        functools.partial(first_kernel, local_heads, block),
        out_shape=(own, other, *packs),
        in_specs=[VMEM_SPEC] * len(inputs),
        out_specs=[VMEM_SPEC] * (2 + len(packs)),
        compiler_params=params(8),
        name="project_0",
    )(*inputs)
    arrived = swap(other, 1)
    parts = pl.pallas_call(
        combine_kernel,
        out_shape=[jax.ShapeDtypeStruct((block, width), BF16)] * blocks,
        in_specs=[VMEM_SPEC] * 2,
        out_specs=[VMEM_SPEC] * blocks,
        compiler_params=params(4),
        cost_estimate=long_cost(),
        name="combine",
    )(own, arrived)
    return parts, packed


def later_kernel(stream_ref, own_ref, other_ref, *out_refs):
    rows, features = stream_ref.shape[0] // 2, stream_ref.shape[1]
    total, squares = 0.0, 0.0
    for k, ref in enumerate((own_ref, other_ref)):
        wide = stream_ref[k * rows : (k + 1) * rows, :].astype(F32)
        pieces = ref[features : features + PIECE, :features].astype(F32)
        gain = pieces[0:1] + pieces[1:2] + pieces[2:3]
        normed = (wide * gain).astype(BF16)
        total = total + dot(normed, ref[:features, :], ((1,), (0,)))
        squares = squares + jnp.sum(wide * wide, axis=-1, keepdims=True)
    at = total.shape[1] - LANES
    tail = in_pieces(with_squares(total[:, at:], squares))
    block = rows // len(out_refs)
    for k, ref in enumerate(out_refs):
        ref[:, :at] = total[k * block : (k + 1) * block, :at].astype(BF16)
        ref[:, at:] = tail[k * block : (k + 1) * block]


def project_later(layer, blocks, stream, own, other):
    rows = stream.shape[0] // 2
    out = jax.ShapeDtypeStruct((rows // blocks, own.shape[1]), BF16)
    return pl.pallas_call(
        later_kernel,
        out_shape=[out] * blocks,
        in_specs=[VMEM_SPEC] * 3,
        out_specs=[VMEM_SPEC] * blocks,
        compiler_params=params(8),
        cost_estimate=long_cost(),
        name=f"project_{layer}",
    )(stream, own, other)


def mix_kernel(
    layer, given, *refs
):
    mix_body(layer, refs[:given], *refs[given:])


def mix_body(
    layer, parts, lengths_ref, taps_ref, bias_ref, alog_ref, skip_ref, gain_ref, past_ref, state_ref,
    mixed_ref, scaled_ref, keys_ref, decay_ref, current_ref,
):
    state, past_ref = state_ref.at[layer], past_ref.at[layer]
    seqs = parts[0].shape[0]
    heads, head_dim, width_n = state.shape[1:]
    width_x = heads * head_dim
    conv = width_x + 2 * width_n
    total = sum(part[...].astype(F32) for part in parts)
    extras = total[:, conv + width_x :]
    extras = extras + pltpu.roll(extras, LANES - PIECE, 1)
    inverse = lax.rsqrt(extras[:, PIECE // 2 : PIECE // 2 + 1] / D + EPSILON)
    current = (total[:, :conv] * inverse).astype(BF16)
    gating = (total[:, conv : conv + width_x] * inverse).astype(BF16).astype(F32)
    current_ref[...] = current

    row = iota((seqs, 1), 0)
    lengths = as_column(lengths_ref)
    taps = taps_ref[layer].astype(F32)
    summed = current.astype(F32) * taps[CONV_W - 1 : CONV_W]
    for j in range(CONV_W - 1):
        past = past_ref[j].astype(F32)
        summed = summed + jnp.where(lengths + j >= CONV_W, past, 0.0) * taps[j : j + 1]
    activated = summed / (1.0 + jnp.exp(-summed))
    head_in = activated[:, :width_x]
    write_keys = activated[:, width_x : width_x + width_n]
    read_keys = activated[:, width_x + width_n :]

    raw = extras[:, :heads] * inverse + bias_ref[layer : layer + 1, :]
    step = jnp.maximum(raw, 0.0) + jnp.log1p(jnp.exp(-jnp.abs(raw)))
    decay = jnp.exp(-jnp.exp(alog_ref[layer : layer + 1, :]) * step)
    decay = jnp.where(lengths >= 2, decay, 0.0)
    lane = iota((seqs, width_x), 1)

    def spread(value):
        out = value[:, 0:1]
        for h in range(1, heads):
            out = jnp.where(lane >= h * head_dim, value[:, h : h + 1], out)
        return out

    scaled = spread(step) * head_in
    scaled_ref[...] = scaled
    keys_ref[...] = write_keys
    decay_ref[...] = decay

    high, low = split(read_keys)
    left = jnp.concatenate(
        [jnp.concatenate([high, high], axis=1), jnp.concatenate([low, jnp.zeros_like(low)], axis=1)], axis=0
    )
    seen = jnp.zeros((seqs, width_x), F32)
    for s in range(seqs):
        old_high, old_low = split(state[s].reshape(width_x, width_n))
        both = dot(left, jnp.concatenate([old_high, old_low], axis=1), ((1,), (1,)))
        seen = jnp.where(row == s, both[:seqs] + both[seqs:], seen)
    pair = jnp.sum(write_keys * read_keys, axis=-1, keepdims=True)
    readout = spread(decay) * seen + scaled * pair + spread(skip_ref[layer : layer + 1, :]) * head_in
    gated = readout * (gating / (1.0 + jnp.exp(-gating)))
    mean = jnp.mean(gated * gated, axis=-1, keepdims=True)
    mixed = (gated * lax.rsqrt(mean + EPSILON) * gain_ref[layer : layer + 1, :]).astype(BF16)
    mixed_ref[...] = mixed


def mix(layer, parts, lengths, taps, bias, alog, skip, gain, past, state):
    seqs = parts[0].shape[-2]
    heads, head_dim, width_n = state.shape[2:]
    width_x = heads * head_dim
    shapes = (
        jax.ShapeDtypeStruct((seqs, width_x), BF16),
        jax.ShapeDtypeStruct((seqs, width_x), F32),
        jax.ShapeDtypeStruct((seqs, width_n), F32),
        jax.ShapeDtypeStruct((seqs, heads), F32),
        jax.ShapeDtypeStruct((seqs, width_x + 2 * width_n), BF16),
    )
    return pl.pallas_call(
        functools.partial(mix_kernel, layer, len(parts)),
        out_shape=shapes,
        in_specs=[*[VMEM_SPEC] * (len(parts) + 8)],
        out_specs=[VMEM_SPEC] * len(shapes),
        compiler_params=params(12),
        name=f"mix_{layer}",
    )(*parts, lengths, taps, bias, alog, skip, gain, past, state)


def output_kernel(layer, given, *refs):
    mixed = jnp.concatenate([ref[...] for ref in refs[:given]], axis=0)
    own_ref, other_ref, out_ref = refs[given:]
    rows = mixed.shape[0]
    for k, ref in enumerate((own_ref, other_ref)):
        out_ref[k * rows : (k + 1) * rows, :] = dot(mixed, ref[layer], ((1,), (0,))).astype(BF16)


def output(layer, mixed, own, other):
    rows = sum(m.shape[0] for m in mixed)
    return pl.pallas_call(
        functools.partial(output_kernel, layer, len(mixed)),
        out_shape=jax.ShapeDtypeStruct((2 * rows, own.shape[2]), BF16),
        in_specs=[VMEM_SPEC] * (len(mixed) + 2),
        out_specs=VMEM_SPEC,
        compiler_params=params(4),
        name=f"output_{layer}",
    )(*mixed, own, other)


def add_kernel(block, parts_ref, *refs):
    streams, out_ref = refs[:-1], refs[-1]
    copies, rows, _ = parts_ref.shape
    total = sum(parts_ref[k].astype(F32) for k in range(copies))
    at = lax.axis_index("tp")
    if len(streams) == 1:
        old = streams[0][pl.ds(pl.multiple_of(at * rows, rows), rows), :]
    else:
        half = copies // 2
        group = lax.rem(at, half)
        per = block // rows
        start = block_at(group // per) * block + lax.rem(group, per) * rows
        first, second = streams
        features = out_ref.shape[-1]
        lowest = second.shape[0] - first.shape[0]
        picked = [
            first[pl.ds(pl.multiple_of(start, rows), rows), :],
            second[pl.ds(pl.multiple_of(lowest + start, rows), rows), :features],
        ]
        old = jnp.where(at < half, picked[0], picked[1])
    new = (old.astype(F32) + total).astype(BF16)
    for k in range(copies):
        out_ref[k] = new


def add(layer, block, parts, streams):
    return pl.pallas_call(
        functools.partial(add_kernel, block),
        out_shape=jax.ShapeDtypeStruct(parts.shape, BF16),
        in_specs=[VMEM_SPEC] * (1 + len(streams)),
        out_specs=VMEM_SPEC,
        compiler_params=params(4),
        name=f"add_{layer}",
    )(parts, *streams)


def order_kernel(block, own_ref, other_ref, out_ref):
    copies, rows, _ = own_ref.shape
    per = block // rows
    half = copies // 2
    for k in range(half // per):
        index = block_at(k)
        for ref, first, at in ((own_ref, 0, index), (other_ref, half, lax.bitwise_xor(index, jnp.int32(1)))):
            value = jnp.concatenate([ref[first + k * per + s] for s in range(per)], axis=0)
            out_ref[pl.ds(pl.multiple_of(at * block, block), block), :] = value


def order(block, own, other):
    copies, rows, features = own.shape
    return pl.pallas_call(
        functools.partial(order_kernel, block),
        out_shape=jax.ShapeDtypeStruct((copies * rows, features), BF16),
        in_specs=[VMEM_SPEC] * 2,
        out_specs=VMEM_SPEC,
        compiler_params=params(4),
        name="order",
    )(own, other)


def states_kernel(layer, pieces, lengths_ref, past_ref, state_ref, scaled_ref, keys_ref, decay_ref, current_ref, *refs):
    conv_ref, new_ref, columns, conv, new, left = refs[-6:]
    seqs, heads, head_dim, width_n = new.shape
    piece = seqs // pieces

    def copy(k):
        rows = pl.ds(k * piece, piece)
        return pltpu.make_async_copy(new.at[rows], new_ref.at[layer, rows], left.at[k])

    scaled = scaled_ref[...]
    rest = jnp.zeros((LANES - seqs, scaled.shape[1]), F32)
    columns[...] = jnp.concatenate([scaled, rest], axis=0).T
    for s in range(seqs):
        for h in range(heads):
            column = columns[h * head_dim : (h + 1) * head_dim, s : s + 1]
            old = decay_ref[s : s + 1, h : h + 1] * state_ref[layer, s, h]
            new[s, h] = old + column * keys_ref[s : s + 1, :]
        if s % piece == 0 and s > 0:
            copy(s // piece - 1).start()
    lengths = as_column(lengths_ref)
    for j in range(1, CONV_W - 1):
        past = past_ref[layer, j].astype(F32)
        conv[j - 1] = jnp.where(lengths + j >= CONV_W, past, 0.0).astype(BF16)
    conv[CONV_W - 2] = current_ref[...]
    copy(pieces - 1).start()
    for k in range(pieces):
        copy(k).wait()
    last = pltpu.make_async_copy(conv, conv_ref.at[layer], left.at[pieces])
    last.start()
    last.wait()


def states(layer, pieces, lengths, past, state, scaled, keys, decay, current, before):
    seqs, heads, head_dim, width_n = state.shape[1:]
    anywhere = pl.BlockSpec(memory_space=pl.ANY)
    inputs = (lengths, past, state, scaled, keys, decay, current)
    return pl.pallas_call(
        functools.partial(states_kernel, layer, pieces),
        out_shape=(jax.ShapeDtypeStruct(past.shape, past.dtype), jax.ShapeDtypeStruct(state.shape, F32)),
        in_specs=[*[VMEM_SPEC] * len(inputs), *[anywhere] * len(before)],
        out_specs=(anywhere, anywhere),
        input_output_aliases={len(inputs) + k: k for k in range(len(before))},
        scratch_shapes=[
            pltpu.VMEM((heads * head_dim, LANES), F32),
            pltpu.VMEM(past.shape[1:], BF16),
            pltpu.VMEM(state.shape[1:], F32),
            pltpu.SemaphoreType.DMA((pieces + 1,)),
        ],
        compiler_params=params(8),
        cost_estimate=pl.CostEstimate(flops=2_000_000_000, bytes_accessed=4 * state.size, transcendentals=0),
        name=f"states_{layer}",
    )(*inputs, *before)


def exchange(blocks, axis):
    return lax.all_to_all(blocks, axis, 0, 0, tiled=True)


def body(
    tokens, lengths, norm_gain, w_z, w_x, w_b, w_c, w_dt, conv_weight, dt_bias, a_log, d_skip, out_gain, w_out,
    conv_state, ssm_state,
):
    tp, dp = lax.axis_size("tp"), lax.axis_size("dp")
    if GROUPS != tp or dp & (dp - 1):
        raise ValueError("unexpected mesh")
    local_heads = HEADS // tp
    rows, features = tokens.shape
    block = rows // dp
    layers = w_z.shape[0]
    w_dt = jnp.swapaxes(w_dt, 1, 2)
    past = jnp.swapaxes(conv_state, 1, 2)
    lengths = lengths.reshape(1, -1)
    across = [2 * k for k in range(1, dp // 2)]

    def over_x(blocks):
        return [blocks[0], *(swap(b, mask) for b, mask in zip(blocks[1:], across))]

    parts, own_packs = project_first(
        local_heads, block, dp // 2, tokens, norm_gain, w_x, w_b, w_c, w_z, w_dt
    )
    parts, own_packs = lax.optimization_barrier((parts, own_packs))
    other_packs = [swap(pack, 1) for pack in own_packs]
    parts = over_x(parts)
    other_out = swap(w_out, 1)
    streams = [tokens, other_packs[0]]
    made = ()
    for layer in range(layers):
        last = layer == layers - 1
        mixed, *rest = mix(
            layer, parts, lengths, conv_weight, dt_bias, a_log, d_skip, out_gain, past, ssm_state
        )
        mixed = over_x([mixed] * (dp // 2))
        if layer == 0:
            mixed, other_packs = lax.optimization_barrier((mixed, other_packs))
        if last:
            made = states(layer, PIECES, lengths, past, ssm_state, *rest, made)
            mixed, made = lax.optimization_barrier((mixed, made))
        share = output(layer, mixed, w_out, other_out)
        share = exchange(share.reshape(tp, rows // tp, features), "tp")
        new = exchange(add(layer, block, share, streams), "tp")
        if not last:
            streams = [new.reshape(rows, features)]
            parts = project_later(
                layer + 1, dp // 2, streams[0], own_packs[layer], other_packs[layer]
            )
            parts, rest = lax.optimization_barrier((parts, rest))
            parts = over_x(parts)
            made = states(layer, PIECES, lengths, past, ssm_state, *rest, made)
            parts, made = lax.optimization_barrier((parts, made))
    conv_new, ssm_new = made
    return order(block, new, swap(new, 1)), jnp.swapaxes(conv_new, 1, 2), ssm_new


def solution(mesh):
    by_seq = ("grp", "dp")
    placed = (
        P("grp", "dp"),
        P(by_seq),
        P(None, "dp"),
        P(None, "dp", "tp"),
        P(None, "dp", "tp"),
        P(None, "dp", "tp"),
        P(None, "dp", "tp"),
        P(None, "dp", None),
        P(None, None, "tp"),
        P(None, "tp"),
        P(None, "tp"),
        P(None, "tp"),
        P(None, "tp"),
        P(None, "tp", "dp"),
        P(None, by_seq, None, "tp"),
        P(None, by_seq, "tp", None, None),
    )
    return jax.shard_map(
        body,
        mesh=mesh,
        in_specs=placed,
        out_specs=(P("grp", "dp"), P(None, by_seq, None, "tp"), P(None, by_seq, "tp", None, None)),
        check_vma=False,
    )
```

```python
import functools

import jax
import jax.numpy as jnp
from jax import lax
from jax.experimental import pallas as pl
from jax.experimental.pallas import tpu as pltpu
from jax.sharding import PartitionSpec as P


D = 4096
HEADS = 64
GROUPS = 16
CONV_W = 4
EPSILON = 1e-06
LANES = 128
PIECE = 16
PIECES = 4
BF16 = jnp.bfloat16
F32 = jnp.float32
MIB = 1 << 20

VMEM_SPEC = pl.BlockSpec(memory_space=pltpu.VMEM)


def params(mib):
    return pltpu.CompilerParams(vmem_limit_bytes=int(mib * MIB))


def iota(shape, dim):
    return lax.broadcasted_iota(jnp.int32, shape, dim)


def dot(a, b, dims):
    return lax.dot_general(a, b, (dims, ((), ())), preferred_element_type=F32)


def as_column(ref):
    count = ref.shape[1]
    same = iota((count, count), 0) == iota((count, count), 1)
    row = jnp.broadcast_to(ref[...].astype(F32), (count, count))
    return jnp.sum(jnp.where(same, row, 0.0), axis=1, keepdims=True)


def split(value):
    high = value.astype(BF16)
    return high, (value - high.astype(F32)).astype(BF16)


def gate_kernel(out_ref):
    out_ref[...] = jnp.zeros_like(out_ref)


def long_cost():
    return pl.CostEstimate(flops=20_000_000_000, bytes_accessed=1_000_000, transcendentals=0)


def gate():
    return pl.pallas_call(
        gate_kernel,
        out_shape=jax.ShapeDtypeStruct((8, LANES), F32),
        out_specs=VMEM_SPEC,
        compiler_params=params(1),
        cost_estimate=long_cost(),
        name="gate",
    )()


def swapped(value, mask):
    pairs = [(i, i ^ mask) for i in range(lax.axis_size("dp"))]
    return lax.ppermute(value, "dp", pairs)


def chosen_heads(heads, local_heads):
    row, column = iota((LANES, heads), 0), iota((LANES, heads), 1)
    local = row % PIECE
    first = lax.axis_index("tp") * local_heads
    return ((column == first + local) & (local < local_heads) & (row < 2 * PIECE)).astype(BF16)


def with_squares(extras, squares):
    return jnp.where(iota(extras.shape, 1) % PIECE == PIECE // 2, squares, extras)


def in_pieces(extras):
    high, low = split(extras)
    return jnp.where(iota(extras.shape, 1) < PIECE, high.astype(F32), low.astype(F32)).astype(BF16)


def block_at(k):
    at = lax.axis_index("dp")
    return lax.bitwise_xor(at // 2, jnp.int32(k)) * 2 + at % 2


def first_kernel(local_heads, block, x_ref, gain_ref, wx_ref, wb_ref, wc_ref, wz_ref, wdt_ref, _, own_ref, other_ref, *packs):
    rows, features = x_ref.shape
    blocks = [block_at(k) for k in range(rows // block // 2)]
    blocks += [lax.bitwise_xor(b, jnp.int32(1)) for b in blocks]
    tokens = [x_ref[pl.ds(pl.multiple_of(b * block, block), block), :] for b in blocks]
    wide = jnp.concatenate(tokens, axis=0).astype(F32)
    normed = (wide * gain_ref[0:1, :]).astype(BF16)
    half = rows // 2
    at = 0
    for ref in (wx_ref, wb_ref, wc_ref, wz_ref):
        width = ref.shape[-1]
        part = dot(normed, ref[0], ((1,), (0,)))
        own_ref[:, at : at + width] = part[:half]
        other_ref[:, at : at + width] = part[half:].astype(BF16)
        at += width
    chosen = chosen_heads(wdt_ref.shape[1], local_heads)
    steps = dot(wdt_ref[0], chosen, ((0,), (1,))).astype(BF16)
    squares = jnp.sum(wide * wide, axis=-1, keepdims=True)
    extras = with_squares(dot(normed, steps, ((1,), (0,))), squares)
    own_ref[:, at:] = extras[:half]
    other_ref[:, at:] = in_pieces(extras[half:])
    for layer, pack in enumerate(packs, 1):
        first = 0
        for ref in (wx_ref, wb_ref, wc_ref, wz_ref):
            pack[:features, first : first + ref.shape[-1]] = ref[layer]
            first += ref.shape[-1]
        pack[:features, at:] = dot(wdt_ref[layer], chosen, ((0,), (1,))).astype(BF16)
        row = iota((PIECE, features), 0)
        left = jnp.broadcast_to(gain_ref[layer : layer + 1, :], row.shape)
        gains = jnp.zeros_like(left)
        for k in range(3):
            piece = left.astype(BF16).astype(F32)
            gains = jnp.where(row == k, piece, gains)
            left = left - piece
        pack[features : features + PIECE, :features] = gains.astype(BF16)
        pack[features + PIECE :, :features] = x_ref[...]


def combine_kernel(own_ref, arrived_ref, *out_refs):
    total = own_ref[...] + arrived_ref[...].astype(F32)
    at = total.shape[1] - LANES
    pieces = arrived_ref[:, at:].astype(F32)
    whole = pieces + pltpu.roll(pieces, LANES - PIECE, 1)
    whole = jnp.where(iota(whole.shape, 1) < PIECE, whole, pltpu.roll(whole, PIECE, 1))
    tail = in_pieces(own_ref[:, at:] + whole)
    block = total.shape[0] // len(out_refs)
    for k, ref in enumerate(out_refs):
        ref[:, :at] = total[k * block : (k + 1) * block, :at].astype(BF16)
        ref[:, at:] = tail[k * block : (k + 1) * block]


def project_first(local_heads, block, blocks, stream, norm_gain, w_x, w_b, w_c, w_z, w_dt):
    rows, features = stream.shape
    width = sum(w.shape[2] for w in (w_x, w_b, w_c, w_z)) + LANES
    own = jax.ShapeDtypeStruct((rows // 2, width), F32)
    other = jax.ShapeDtypeStruct((rows // 2, width), BF16)
    packs = [jax.ShapeDtypeStruct((features + PIECE + rows, width), BF16)] * (w_z.shape[0] - 1)
    inputs = [stream, norm_gain, w_x, w_b, w_c, w_z, w_dt, gate()]
    own, other, *packed = pl.pallas_call(
        functools.partial(first_kernel, local_heads, block),
        out_shape=(own, other, *packs),
        in_specs=[VMEM_SPEC] * len(inputs),
        out_specs=[VMEM_SPEC] * (2 + len(packs)),
        compiler_params=params(8),
        name="project_0",
    )(*inputs)
    arrived = swapped(other, 1)
    parts = pl.pallas_call(
        combine_kernel,
        out_shape=[jax.ShapeDtypeStruct((block, width), BF16)] * blocks,
        in_specs=[VMEM_SPEC] * 2,
        out_specs=[VMEM_SPEC] * blocks,
        compiler_params=params(4),
        cost_estimate=long_cost(),
        name="combine",
    )(own, arrived)
    return parts, packed


def later_kernel(stream_ref, own_ref, other_ref, *out_refs):
    rows, features = stream_ref.shape[0] // 2, stream_ref.shape[1]
    total, squares = 0.0, 0.0
    for k, ref in enumerate((own_ref, other_ref)):
        wide = stream_ref[k * rows : (k + 1) * rows, :].astype(F32)
        pieces = ref[features : features + PIECE, :features].astype(F32)
        gain = pieces[0:1] + pieces[1:2] + pieces[2:3]
        normed = (wide * gain).astype(BF16)
        total = total + dot(normed, ref[:features, :], ((1,), (0,)))
        squares = squares + jnp.sum(wide * wide, axis=-1, keepdims=True)
    at = total.shape[1] - LANES
    tail = in_pieces(with_squares(total[:, at:], squares))
    block = rows // len(out_refs)
    for k, ref in enumerate(out_refs):
        ref[:, :at] = total[k * block : (k + 1) * block, :at].astype(BF16)
        ref[:, at:] = tail[k * block : (k + 1) * block]


def project_later(blocks, stream, own, other):
    rows = stream.shape[0] // 2
    out = jax.ShapeDtypeStruct((rows // blocks, own.shape[1]), BF16)
    return pl.pallas_call(
        later_kernel,
        out_shape=[out] * blocks,
        in_specs=[VMEM_SPEC] * 3,
        out_specs=[VMEM_SPEC] * blocks,
        compiler_params=params(8),
        cost_estimate=long_cost(),
    )(stream, own, other)


def mix_kernel(
    layer, given, *refs
):
    mix_body(layer, refs[:given], *refs[given:])


def mix_body(
    layer, parts, lengths_ref, taps_ref, bias_ref, alog_ref, skip_ref, gain_ref, past_ref, state_ref,
    mixed_ref, scaled_ref, keys_ref, decay_ref, current_ref,
):
    state, past_ref = state_ref.at[layer], past_ref.at[layer]
    seqs = parts[0].shape[0]
    heads, head_dim, width_n = state.shape[1:]
    width_x = heads * head_dim
    conv = width_x + 2 * width_n
    total = sum(part[...].astype(F32) for part in parts)
    extras = total[:, conv + width_x :]
    extras = extras + pltpu.roll(extras, LANES - PIECE, 1)
    inverse = lax.rsqrt(extras[:, PIECE // 2 : PIECE // 2 + 1] / D + EPSILON)
    current = (total[:, :conv] * inverse).astype(BF16)
    gating = (total[:, conv : conv + width_x] * inverse).astype(BF16).astype(F32)
    current_ref[...] = current

    row = iota((seqs, 1), 0)
    lengths = as_column(lengths_ref)
    taps = taps_ref[layer].astype(F32)
    summed = current.astype(F32) * taps[CONV_W - 1 : CONV_W]
    for j in range(CONV_W - 1):
        past = past_ref[j].astype(F32)
        summed = summed + jnp.where(lengths + j >= CONV_W, past, 0.0) * taps[j : j + 1]
    activated = summed / (1.0 + jnp.exp(-summed))
    head_in = activated[:, :width_x]
    write_keys = activated[:, width_x : width_x + width_n]
    read_keys = activated[:, width_x + width_n :]

    raw = extras[:, :heads] * inverse + bias_ref[layer : layer + 1, :]
    step = jnp.maximum(raw, 0.0) + jnp.log1p(jnp.exp(-jnp.abs(raw)))
    decay = jnp.exp(-jnp.exp(alog_ref[layer : layer + 1, :]) * step)
    decay = jnp.where(lengths >= 2, decay, 0.0)
    lane = iota((seqs, width_x), 1)

    def spread(value):
        out = value[:, 0:1]
        for h in range(1, heads):
            out = jnp.where(lane >= h * head_dim, value[:, h : h + 1], out)
        return out

    scaled = spread(step) * head_in
    scaled_ref[...] = scaled
    keys_ref[...] = write_keys
    decay_ref[...] = decay

    high, low = split(read_keys)
    left = jnp.concatenate(
        [jnp.concatenate([high, high], axis=1), jnp.concatenate([low, jnp.zeros_like(low)], axis=1)], axis=0
    )
    seen = jnp.zeros((seqs, width_x), F32)
    for s in range(seqs):
        old_high, old_low = split(state[s].reshape(width_x, width_n))
        both = dot(left, jnp.concatenate([old_high, old_low], axis=1), ((1,), (1,)))
        seen = jnp.where(row == s, both[:seqs] + both[seqs:], seen)
    pair = jnp.sum(write_keys * read_keys, axis=-1, keepdims=True)
    readout = spread(decay) * seen + scaled * pair + spread(skip_ref[layer : layer + 1, :]) * head_in
    gated = readout * (gating / (1.0 + jnp.exp(-gating)))
    mean = jnp.mean(gated * gated, axis=-1, keepdims=True)
    mixed = (gated * lax.rsqrt(mean + EPSILON) * gain_ref[layer : layer + 1, :]).astype(BF16)
    mixed_ref[...] = mixed


def mix(layer, parts, lengths, taps, bias, alog, skip, gain, past, state):
    seqs = parts[0].shape[-2]
    heads, head_dim, width_n = state.shape[2:]
    width_x = heads * head_dim
    shapes = (
        jax.ShapeDtypeStruct((seqs, width_x), BF16),
        jax.ShapeDtypeStruct((seqs, width_x), F32),
        jax.ShapeDtypeStruct((seqs, width_n), F32),
        jax.ShapeDtypeStruct((seqs, heads), F32),
        jax.ShapeDtypeStruct((seqs, width_x + 2 * width_n), BF16),
    )
    return pl.pallas_call(
        functools.partial(mix_kernel, layer, len(parts)),
        out_shape=shapes,
        in_specs=[*[VMEM_SPEC] * (len(parts) + 8)],
        out_specs=[VMEM_SPEC] * len(shapes),
        compiler_params=params(12),
    )(*parts, lengths, taps, bias, alog, skip, gain, past, state)


def output_kernel(layer, given, *refs):
    mixed = jnp.concatenate([ref[...] for ref in refs[:given]], axis=0)
    own_ref, other_ref, out_ref = refs[given:]
    rows = mixed.shape[0]
    for k, ref in enumerate((own_ref, other_ref)):
        out_ref[k * rows : (k + 1) * rows, :] = dot(mixed, ref[layer], ((1,), (0,))).astype(BF16)


def output(layer, mixed, own, other):
    rows = sum(m.shape[0] for m in mixed)
    return pl.pallas_call(
        functools.partial(output_kernel, layer, len(mixed)),
        out_shape=jax.ShapeDtypeStruct((2 * rows, own.shape[2]), BF16),
        in_specs=[VMEM_SPEC] * (len(mixed) + 2),
        out_specs=VMEM_SPEC,
        compiler_params=params(4),
    )(*mixed, own, other)


def add_kernel(block, parts_ref, *refs):
    streams, out_ref = refs[:-1], refs[-1]
    copies, rows, _ = parts_ref.shape
    total = sum(parts_ref[k].astype(F32) for k in range(copies))
    at = lax.axis_index("tp")
    if len(streams) == 1:
        old = streams[0][pl.ds(pl.multiple_of(at * rows, rows), rows), :]
    else:
        half = copies // 2
        group = lax.rem(at, half)
        per = block // rows
        start = block_at(group // per) * block + lax.rem(group, per) * rows
        first, second = streams
        features = out_ref.shape[-1]
        lowest = second.shape[0] - first.shape[0]
        picked = [
            first[pl.ds(pl.multiple_of(start, rows), rows), :],
            second[pl.ds(pl.multiple_of(lowest + start, rows), rows), :features],
        ]
        old = jnp.where(at < half, picked[0], picked[1])
    new = (old.astype(F32) + total).astype(BF16)
    for k in range(copies):
        out_ref[k] = new


def add(block, parts, streams):
    return pl.pallas_call(
        functools.partial(add_kernel, block),
        out_shape=jax.ShapeDtypeStruct(parts.shape, BF16),
        in_specs=[VMEM_SPEC] * (1 + len(streams)),
        out_specs=VMEM_SPEC,
        compiler_params=params(4),
    )(parts, *streams)


def order_kernel(block, own_ref, other_ref, out_ref):
    copies, rows, _ = own_ref.shape
    per = block // rows
    half = copies // 2
    for k in range(half // per):
        index = block_at(k)
        for ref, at in ((own_ref, index), (other_ref, lax.bitwise_xor(index, jnp.int32(1)))):
            value = jnp.concatenate([ref[k * per + s] for s in range(per)], axis=0)
            out_ref[pl.ds(pl.multiple_of(at * block, block), block), :] = value


def order(block, own, other):
    copies, rows, features = own.shape
    return pl.pallas_call(
        functools.partial(order_kernel, block),
        out_shape=jax.ShapeDtypeStruct((copies * rows, features), BF16),
        in_specs=[VMEM_SPEC] * 2,
        out_specs=VMEM_SPEC,
        compiler_params=params(4),
        name="order",
    )(own, other)


def states_kernel(layer, pieces, lengths_ref, past_ref, state_ref, scaled_ref, keys_ref, decay_ref, current_ref, *refs):
    conv_ref, new_ref, columns, conv, new, left = refs[-6:]
    seqs, heads, head_dim, _ = new.shape
    piece = seqs // pieces

    def copy(k):
        rows = pl.ds(k * piece, piece)
        return pltpu.make_async_copy(new.at[rows], new_ref.at[layer, rows], left.at[k])

    scaled = scaled_ref[...]
    rest = jnp.zeros((LANES - seqs, scaled.shape[1]), F32)
    columns[...] = jnp.concatenate([scaled, rest], axis=0).T
    for s in range(seqs):
        for h in range(heads):
            column = columns[h * head_dim : (h + 1) * head_dim, s : s + 1]
            old = decay_ref[s : s + 1, h : h + 1] * state_ref[layer, s, h]
            new[s, h] = old + column * keys_ref[s : s + 1, :]
        if s % piece == 0 and s > 0:
            copy(s // piece - 1).start()
    lengths = as_column(lengths_ref)
    for j in range(1, CONV_W - 1):
        past = past_ref[layer, j].astype(F32)
        conv[j - 1] = jnp.where(lengths + j >= CONV_W, past, 0.0).astype(BF16)
    conv[CONV_W - 2] = current_ref[...]
    copy(pieces - 1).start()
    for k in range(pieces):
        copy(k).wait()
    last = pltpu.make_async_copy(conv, conv_ref.at[layer], left.at[pieces])
    last.start()
    last.wait()


def states(layer, pieces, lengths, past, state, scaled, keys, decay, current, before):
    _, heads, head_dim, _ = state.shape[1:]
    anywhere = pl.BlockSpec(memory_space=pl.ANY)
    inputs = (lengths, past, state, scaled, keys, decay, current)
    return pl.pallas_call(
        functools.partial(states_kernel, layer, pieces),
        out_shape=(jax.ShapeDtypeStruct(past.shape, past.dtype), jax.ShapeDtypeStruct(state.shape, F32)),
        in_specs=[*[VMEM_SPEC] * len(inputs), *[anywhere] * len(before)],
        out_specs=(anywhere, anywhere),
        input_output_aliases={len(inputs) + k: k for k in range(len(before))},
        scratch_shapes=[
            pltpu.VMEM((heads * head_dim, LANES), F32),
            pltpu.VMEM(past.shape[1:], BF16),
            pltpu.VMEM(state.shape[1:], F32),
            pltpu.SemaphoreType.DMA((pieces + 1,)),
        ],
        compiler_params=params(8),
        cost_estimate=pl.CostEstimate(flops=2_000_000_000, bytes_accessed=4 * state.size, transcendentals=0),
    )(*inputs, *before)


def exchange(blocks, axis):
    return lax.all_to_all(blocks, axis, 0, 0, tiled=True)


def body(
    tokens, lengths, norm_gain, w_z, w_x, w_b, w_c, w_dt, conv_weight, dt_bias, a_log, d_skip, out_gain, w_out,
    conv_state, ssm_state,
):
    tp, dp = lax.axis_size("tp"), lax.axis_size("dp")
    if GROUPS != tp or dp & (dp - 1):
        raise ValueError("unexpected mesh")
    local_heads = HEADS // tp
    rows, features = tokens.shape
    block = rows // dp
    layers = w_z.shape[0]
    w_dt = jnp.swapaxes(w_dt, 1, 2)
    past = jnp.swapaxes(conv_state, 1, 2)
    lengths = lengths.reshape(1, -1)
    across = [2 * k for k in range(1, dp // 2)]

    def over_x(blocks):
        return [blocks[0], *(swapped(b, mask) for b, mask in zip(blocks[1:], across))]

    parts, own_packs = project_first(
        local_heads, block, dp // 2, tokens, norm_gain, w_x, w_b, w_c, w_z, w_dt
    )
    other_packs = [swapped(pack, 1) for pack in own_packs]
    parts = over_x(parts)
    other_out = swapped(w_out, 1)
    streams = [tokens, other_packs[0]]
    made = ()
    for layer in range(layers):
        last = layer == layers - 1
        mixed, *rest = mix(
            layer, parts, lengths, conv_weight, dt_bias, a_log, d_skip, out_gain, past, ssm_state
        )
        mixed = over_x([mixed] * (dp // 2))
        if layer == 0:
            mixed, other_packs = lax.optimization_barrier((mixed, other_packs))
        if last:
            made = states(layer, PIECES, lengths, past, ssm_state, *rest, made)
            mixed, made = lax.optimization_barrier((mixed, made))
        share = output(layer, mixed, w_out, other_out)
        share = exchange(share.reshape(tp, rows // tp, features), "tp")
        new = exchange(add(block, share, streams), "tp")
        if not last:
            streams = [new.reshape(rows, features)]
            parts = project_later(dp // 2, streams[0], own_packs[layer], other_packs[layer])
            parts, rest = lax.optimization_barrier((parts, rest))
            parts = over_x(parts)
            made = states(layer, PIECES, lengths, past, ssm_state, *rest, made)
            parts, made = lax.optimization_barrier((parts, made))
    conv_new, ssm_new = made
    return order(block, new, swapped(new[tp // 2 :], 1)), jnp.swapaxes(conv_new, 1, 2), ssm_new


def solution(mesh):
    by_seq = ("grp", "dp")
    placed = (
        P("grp", "dp"),
        P(by_seq),
        P(None, "dp"),
        P(None, "dp", "tp"),
        P(None, "dp", "tp"),
        P(None, "dp", "tp"),
        P(None, "dp", "tp"),
        P(None, "dp", None),
        P(None, None, "tp"),
        P(None, "tp"),
        P(None, "tp"),
        P(None, "tp"),
        P(None, "tp"),
        P(None, "tp", "dp"),
        P(None, by_seq, None, "tp"),
        P(None, by_seq, "tp", None, None),
    )
    return jax.shard_map(
        body,
        mesh=mesh,
        in_specs=placed,
        out_specs=(P("grp", "dp"), P(None, by_seq, None, "tp"), P(None, by_seq, "tp", None, None)),
        check_vma=False,
    )
```

```python
import functools

import jax
import jax.numpy as jnp
from jax import lax
from jax.experimental import pallas as pl
from jax.experimental.pallas import tpu as pltpu
from jax.sharding import PartitionSpec as P


D = 4096
HEADS = 64
GROUPS = 16
CONV_W = 4
EPSILON = 1e-06
LANES = 128
PIECE = 16
PIECES = 4
BF16 = jnp.bfloat16
F32 = jnp.float32
MIB = 1 << 20

VMEM_SPEC = pl.BlockSpec(memory_space=pltpu.VMEM)


def params(mib):
    return pltpu.CompilerParams(vmem_limit_bytes=int(mib * MIB))


def iota(shape, dim):
    return lax.broadcasted_iota(jnp.int32, shape, dim)


def dot(a, b, dims):
    return lax.dot_general(a, b, (dims, ((), ())), preferred_element_type=F32)


def as_column(ref):
    count = ref.shape[1]
    same = iota((count, count), 0) == iota((count, count), 1)
    row = jnp.broadcast_to(ref[...].astype(F32), (count, count))
    return jnp.sum(jnp.where(same, row, 0.0), axis=1, keepdims=True)


def split(value):
    high = value.astype(BF16)
    return high, (value - high.astype(F32)).astype(BF16)


def gate_kernel(out_ref):
    out_ref[...] = jnp.zeros_like(out_ref)


def long_cost():
    return pl.CostEstimate(flops=20_000_000_000, bytes_accessed=1_000_000, transcendentals=0)


def gate():
    return pl.pallas_call(
        gate_kernel,
        out_shape=jax.ShapeDtypeStruct((8, LANES), F32),
        out_specs=VMEM_SPEC,
        compiler_params=params(1),
        cost_estimate=long_cost(),
        name="gate",
    )()


def swapped(value, mask):
    pairs = [(i, i ^ mask) for i in range(lax.axis_size("dp"))]
    return lax.ppermute(value, "dp", pairs)


def chosen_heads(heads, local_heads):
    row, column = iota((LANES, heads), 0), iota((LANES, heads), 1)
    local = row % PIECE
    first = lax.axis_index("tp") * local_heads
    return ((column == first + local) & (local < local_heads) & (row < 2 * PIECE)).astype(BF16)


def with_squares(extras, squares):
    return jnp.where(iota(extras.shape, 1) % PIECE == PIECE // 2, squares, extras)


def in_pieces(extras):
    high, low = split(extras)
    return jnp.where(iota(extras.shape, 1) < PIECE, high.astype(F32), low.astype(F32)).astype(BF16)


def block_at(k):
    at = lax.axis_index("dp")
    return lax.bitwise_xor(at // 2, jnp.int32(k)) * 2 + at % 2


def first_rows(local_heads, block, away, x_ref, gain_ref, weights, wdt_ref, out_ref):
    half = x_ref.shape[0] // 2
    blocks = [lax.bitwise_xor(block_at(k), jnp.int32(away)) for k in range(half // block)]
    tokens = [x_ref[pl.ds(pl.multiple_of(b * block, block), block), :] for b in blocks]
    wide = jnp.concatenate(tokens, axis=0).astype(F32)
    normed = (wide * gain_ref[0:1, :]).astype(BF16)
    at = 0
    for ref in weights:
        width = ref.shape[-1]
        out_ref[:, at : at + width] = dot(normed, ref[0], ((1,), (0,))).astype(out_ref.dtype)
        at += width
    chosen = chosen_heads(wdt_ref.shape[1], local_heads)
    steps = dot(wdt_ref[0], chosen, ((0,), (1,))).astype(BF16)
    squares = jnp.sum(wide * wide, axis=-1, keepdims=True)
    extras = with_squares(dot(normed, steps, ((1,), (0,))), squares)
    out_ref[:, at:] = in_pieces(extras) if away else extras


def away_kernel(local_heads, block, x_ref, gain_ref, wx_ref, wb_ref, wc_ref, wz_ref, wdt_ref, _, out_ref):
    first_rows(local_heads, block, 1, x_ref, gain_ref, (wx_ref, wb_ref, wc_ref, wz_ref), wdt_ref, out_ref)


def home_kernel(local_heads, block, x_ref, gain_ref, wx_ref, wb_ref, wc_ref, wz_ref, wdt_ref, own_ref, *packs):
    weights = (wx_ref, wb_ref, wc_ref, wz_ref)
    first_rows(local_heads, block, 0, x_ref, gain_ref, weights, wdt_ref, own_ref)
    features = x_ref.shape[1]
    at = own_ref.shape[1] - LANES
    chosen = chosen_heads(wdt_ref.shape[1], local_heads)
    for layer, pack in enumerate(packs, 1):
        first = 0
        for ref in weights:
            pack[:features, first : first + ref.shape[-1]] = ref[layer]
            first += ref.shape[-1]
        pack[:features, at:] = dot(wdt_ref[layer], chosen, ((0,), (1,))).astype(BF16)
        row = iota((PIECE, features), 0)
        left = jnp.broadcast_to(gain_ref[layer : layer + 1, :], row.shape)
        gains = jnp.zeros_like(left)
        for k in range(3):
            piece = left.astype(BF16).astype(F32)
            gains = jnp.where(row == k, piece, gains)
            left = left - piece
        pack[features : features + PIECE, :features] = gains.astype(BF16)
        pack[features + PIECE :, :features] = x_ref[...]


def combine_kernel(own_ref, arrived_ref, *out_refs):
    total = own_ref[...] + arrived_ref[...].astype(F32)
    at = total.shape[1] - LANES
    pieces = arrived_ref[:, at:].astype(F32)
    whole = pieces + pltpu.roll(pieces, LANES - PIECE, 1)
    whole = jnp.where(iota(whole.shape, 1) < PIECE, whole, pltpu.roll(whole, PIECE, 1))
    tail = in_pieces(own_ref[:, at:] + whole)
    block = total.shape[0] // len(out_refs)
    for k, ref in enumerate(out_refs):
        ref[:, :at] = total[k * block : (k + 1) * block, :at].astype(BF16)
        ref[:, at:] = tail[k * block : (k + 1) * block]


def project_first(local_heads, block, blocks, stream, norm_gain, w_x, w_b, w_c, w_z, w_dt):
    rows, features = stream.shape
    width = sum(w.shape[2] for w in (w_x, w_b, w_c, w_z)) + LANES
    own = jax.ShapeDtypeStruct((rows // 2, width), F32)
    other = jax.ShapeDtypeStruct((rows // 2, width), BF16)
    packs = [jax.ShapeDtypeStruct((features + PIECE + rows, width), BF16)] * (w_z.shape[0] - 1)
    inputs = [stream, norm_gain, w_x, w_b, w_c, w_z, w_dt]
    other = pl.pallas_call(
        functools.partial(away_kernel, local_heads, block),
        out_shape=other,
        in_specs=[VMEM_SPEC] * (1 + len(inputs)),
        out_specs=VMEM_SPEC,
        compiler_params=params(8),
        name="project_away",
    )(*inputs, gate())
    own, *packed = pl.pallas_call(
        functools.partial(home_kernel, local_heads, block),
        out_shape=(own, *packs),
        in_specs=[VMEM_SPEC] * len(inputs),
        out_specs=[VMEM_SPEC] * (1 + len(packs)),
        compiler_params=params(8),
        cost_estimate=pl.CostEstimate(flops=200_000_000, bytes_accessed=2_000_000, transcendentals=0),
        name="project_home",
    )(*inputs)
    arrived = swapped(other, 1)
    parts = pl.pallas_call(
        combine_kernel,
        out_shape=[jax.ShapeDtypeStruct((block, width), BF16)] * blocks,
        in_specs=[VMEM_SPEC] * 2,
        out_specs=[VMEM_SPEC] * blocks,
        compiler_params=params(4),
        cost_estimate=long_cost(),
        name="combine",
    )(own, arrived)
    return parts, packed


def later_kernel(stream_ref, own_ref, other_ref, *out_refs):
    rows, features = stream_ref.shape[0] // 2, stream_ref.shape[1]
    total, squares = 0.0, 0.0
    for k, ref in enumerate((own_ref, other_ref)):
        wide = stream_ref[k * rows : (k + 1) * rows, :].astype(F32)
        pieces = ref[features : features + PIECE, :features].astype(F32)
        gain = pieces[0:1] + pieces[1:2] + pieces[2:3]
        normed = (wide * gain).astype(BF16)
        total = total + dot(normed, ref[:features, :], ((1,), (0,)))
        squares = squares + jnp.sum(wide * wide, axis=-1, keepdims=True)
    at = total.shape[1] - LANES
    tail = in_pieces(with_squares(total[:, at:], squares))
    block = rows // len(out_refs)
    for k, ref in enumerate(out_refs):
        ref[:, :at] = total[k * block : (k + 1) * block, :at].astype(BF16)
        ref[:, at:] = tail[k * block : (k + 1) * block]


def project_later(blocks, stream, own, other):
    rows = stream.shape[0] // 2
    out = jax.ShapeDtypeStruct((rows // blocks, own.shape[1]), BF16)
    return pl.pallas_call(
        later_kernel,
        out_shape=[out] * blocks,
        in_specs=[VMEM_SPEC] * 3,
        out_specs=[VMEM_SPEC] * blocks,
        compiler_params=params(8),
        cost_estimate=long_cost(),
    )(stream, own, other)


def mix_kernel(
    layer, given, *refs
):
    mix_body(layer, refs[:given], *refs[given:])


def mix_body(
    layer, parts, lengths_ref, taps_ref, bias_ref, alog_ref, skip_ref, gain_ref, past_ref, state_ref,
    mixed_ref, scaled_ref, keys_ref, decay_ref, current_ref,
):
    past_ref = past_ref.at[layer]
    seqs = parts[0].shape[0]
    heads = bias_ref.shape[1]
    width_x, width_n = state_ref.shape[2], state_ref.shape[3] // 2
    head_dim = width_x // heads
    conv = width_x + 2 * width_n
    total = sum(part[...].astype(F32) for part in parts)
    extras = total[:, conv + width_x :]
    extras = extras + pltpu.roll(extras, LANES - PIECE, 1)
    inverse = lax.rsqrt(extras[:, PIECE // 2 : PIECE // 2 + 1] / D + EPSILON)
    current = (total[:, :conv] * inverse).astype(BF16)
    gating = (total[:, conv : conv + width_x] * inverse).astype(BF16).astype(F32)
    current_ref[...] = current

    row = iota((seqs, 1), 0)
    lengths = as_column(lengths_ref)
    taps = taps_ref[layer].astype(F32)
    summed = current.astype(F32) * taps[CONV_W - 1 : CONV_W]
    for j in range(CONV_W - 1):
        past = past_ref[j].astype(F32)
        summed = summed + jnp.where(lengths + j >= CONV_W, past, 0.0) * taps[j : j + 1]
    activated = summed / (1.0 + jnp.exp(-summed))
    head_in = activated[:, :width_x]
    write_keys = activated[:, width_x : width_x + width_n]
    read_keys = activated[:, width_x + width_n :]

    raw = extras[:, :heads] * inverse + bias_ref[layer : layer + 1, :]
    step = jnp.maximum(raw, 0.0) + jnp.log1p(jnp.exp(-jnp.abs(raw)))
    decay = jnp.exp(-jnp.exp(alog_ref[layer : layer + 1, :]) * step)
    decay = jnp.where(lengths >= 2, decay, 0.0)
    lane = iota((seqs, width_x), 1)

    def spread(value):
        out = value[:, 0:1]
        for h in range(1, heads):
            out = jnp.where(lane >= h * head_dim, value[:, h : h + 1], out)
        return out

    scaled = spread(step) * head_in
    scaled_ref[...] = scaled
    keys_ref[...] = write_keys
    decay_ref[...] = decay

    high, low = split(read_keys)
    left = jnp.concatenate(
        [jnp.concatenate([high, high], axis=1), jnp.concatenate([low, jnp.zeros_like(low)], axis=1)], axis=0
    )
    seen = jnp.zeros((seqs, width_x), F32)
    for s in range(seqs):
        both = dot(left, state_ref[layer, s], ((1,), (1,)))
        seen = jnp.where(row == s, both[:seqs] + both[seqs:], seen)
    pair = jnp.sum(write_keys * read_keys, axis=-1, keepdims=True)
    readout = spread(decay) * seen + scaled * pair + spread(skip_ref[layer : layer + 1, :]) * head_in
    gated = readout * (gating / (1.0 + jnp.exp(-gating)))
    mean = jnp.mean(gated * gated, axis=-1, keepdims=True)
    mixed = (gated * lax.rsqrt(mean + EPSILON) * gain_ref[layer : layer + 1, :]).astype(BF16)
    mixed_ref[...] = mixed


def mix(layer, parts, lengths, taps, bias, alog, skip, gain, past, state):
    seqs = parts[0].shape[-2]
    heads, width_x, width_n = bias.shape[1], state.shape[2], state.shape[3] // 2
    shapes = (
        jax.ShapeDtypeStruct((seqs, width_x), BF16),
        jax.ShapeDtypeStruct((seqs, width_x), F32),
        jax.ShapeDtypeStruct((seqs, width_n), F32),
        jax.ShapeDtypeStruct((seqs, heads), F32),
        jax.ShapeDtypeStruct((seqs, width_x + 2 * width_n), BF16),
    )
    return pl.pallas_call(
        functools.partial(mix_kernel, layer, len(parts)),
        out_shape=shapes,
        in_specs=[*[VMEM_SPEC] * (len(parts) + 8)],
        out_specs=[VMEM_SPEC] * len(shapes),
        compiler_params=params(12),
    )(*parts, lengths, taps, bias, alog, skip, gain, past, state)


def output_kernel(layer, given, *refs):
    mixed = jnp.concatenate([ref[...] for ref in refs[:given]], axis=0)
    own_ref, other_ref, out_ref = refs[given:]
    rows = mixed.shape[0]
    for k, ref in enumerate((own_ref, other_ref)):
        out_ref[k * rows : (k + 1) * rows, :] = dot(mixed, ref[layer], ((1,), (0,))).astype(BF16)


def output(layer, mixed, own, other):
    rows = sum(m.shape[0] for m in mixed)
    return pl.pallas_call(
        functools.partial(output_kernel, layer, len(mixed)),
        out_shape=jax.ShapeDtypeStruct((2 * rows, own.shape[2]), BF16),
        in_specs=[VMEM_SPEC] * (len(mixed) + 2),
        out_specs=VMEM_SPEC,
        compiler_params=params(4),
    )(*mixed, own, other)


def add_kernel(block, parts_ref, *refs):
    streams, out_ref = refs[:-1], refs[-1]
    copies, rows, _ = parts_ref.shape
    total = sum(parts_ref[k].astype(F32) for k in range(copies))
    at = lax.axis_index("tp")
    if len(streams) == 1:
        old = streams[0][pl.ds(pl.multiple_of(at * rows, rows), rows), :]
    else:
        half = copies // 2
        group = lax.rem(at, half)
        per = block // rows
        start = block_at(group // per) * block + lax.rem(group, per) * rows
        first, second = streams
        features = out_ref.shape[-1]
        lowest = second.shape[0] - first.shape[0]
        picked = [
            first[pl.ds(pl.multiple_of(start, rows), rows), :],
            second[pl.ds(pl.multiple_of(lowest + start, rows), rows), :features],
        ]
        old = jnp.where(at < half, picked[0], picked[1])
    new = (old.astype(F32) + total).astype(BF16)
    for k in range(copies):
        out_ref[k] = new


def add(block, parts, streams):
    return pl.pallas_call(
        functools.partial(add_kernel, block),
        out_shape=jax.ShapeDtypeStruct(parts.shape, BF16),
        in_specs=[VMEM_SPEC] * (1 + len(streams)),
        out_specs=VMEM_SPEC,
        compiler_params=params(4),
    )(parts, *streams)


def order_kernel(block, own_ref, other_ref, out_ref):
    copies, rows, _ = own_ref.shape
    per = block // rows
    half = copies // 2
    for k in range(half // per):
        index = block_at(k)
        for ref, at in ((own_ref, index), (other_ref, lax.bitwise_xor(index, jnp.int32(1)))):
            value = jnp.concatenate([ref[k * per + s] for s in range(per)], axis=0)
            out_ref[pl.ds(pl.multiple_of(at * block, block), block), :] = value


def order(block, own, other):
    copies, rows, features = own.shape
    return pl.pallas_call(
        functools.partial(order_kernel, block),
        out_shape=jax.ShapeDtypeStruct((copies * rows, features), BF16),
        in_specs=[VMEM_SPEC] * 2,
        out_specs=VMEM_SPEC,
        compiler_params=params(4),
        name="order",
    )(own, other)


def prepare_kernel(_, state_ref, out_ref):
    layers, seqs, heads, head_dim, width_n = state_ref.shape
    for layer in range(layers):
        for s in range(seqs):
            high, low = split(state_ref[layer, s].reshape(heads * head_dim, width_n))
            out_ref[layer, s, :, :width_n] = high
            out_ref[layer, s, :, width_n:] = low


def prepare(after, state):
    layers, seqs, heads, head_dim, width_n = state.shape
    return pl.pallas_call(
        prepare_kernel,
        out_shape=jax.ShapeDtypeStruct((layers, seqs, heads * head_dim, 2 * width_n), BF16),
        in_specs=[VMEM_SPEC] * 2,
        out_specs=VMEM_SPEC,
        compiler_params=params(12),
        cost_estimate=pl.CostEstimate(flops=500_000_000, bytes_accessed=2 * state.size, transcendentals=0),
        name="prepare",
    )(after, state)


def states_kernel(layer, pieces, lengths_ref, past_ref, state_ref, scaled_ref, keys_ref, decay_ref, current_ref, *refs):
    conv_ref, new_ref, columns, conv, new, left = refs[-6:]
    seqs, heads, head_dim, _ = new.shape
    piece = seqs // pieces

    def copy(k):
        rows = pl.ds(k * piece, piece)
        return pltpu.make_async_copy(new.at[rows], new_ref.at[layer, rows], left.at[k])

    scaled = scaled_ref[...]
    rest = jnp.zeros((LANES - seqs, scaled.shape[1]), F32)
    columns[...] = jnp.concatenate([scaled, rest], axis=0).T
    for s in range(seqs):
        for h in range(heads):
            column = columns[h * head_dim : (h + 1) * head_dim, s : s + 1]
            old = decay_ref[s : s + 1, h : h + 1] * state_ref[layer, s, h]
            new[s, h] = old + column * keys_ref[s : s + 1, :]
        if s % piece == 0 and s > 0:
            copy(s // piece - 1).start()
    lengths = as_column(lengths_ref)
    for j in range(1, CONV_W - 1):
        past = past_ref[layer, j].astype(F32)
        conv[j - 1] = jnp.where(lengths + j >= CONV_W, past, 0.0).astype(BF16)
    conv[CONV_W - 2] = current_ref[...]
    copy(pieces - 1).start()
    for k in range(pieces):
        copy(k).wait()
    last = pltpu.make_async_copy(conv, conv_ref.at[layer], left.at[pieces])
    last.start()
    last.wait()


def states(layer, pieces, lengths, past, state, scaled, keys, decay, current, before):
    _, heads, head_dim, _ = state.shape[1:]
    anywhere = pl.BlockSpec(memory_space=pl.ANY)
    inputs = (lengths, past, state, scaled, keys, decay, current)
    return pl.pallas_call(
        functools.partial(states_kernel, layer, pieces),
        out_shape=(jax.ShapeDtypeStruct(past.shape, past.dtype), jax.ShapeDtypeStruct(state.shape, F32)),
        in_specs=[*[VMEM_SPEC] * len(inputs), *[anywhere] * len(before)],
        out_specs=(anywhere, anywhere),
        input_output_aliases={len(inputs) + k: k for k in range(len(before))},
        scratch_shapes=[
            pltpu.VMEM((heads * head_dim, LANES), F32),
            pltpu.VMEM(past.shape[1:], BF16),
            pltpu.VMEM(state.shape[1:], F32),
            pltpu.SemaphoreType.DMA((pieces + 1,)),
        ],
        compiler_params=params(8),
        cost_estimate=pl.CostEstimate(flops=2_000_000_000, bytes_accessed=4 * state.size, transcendentals=0),
    )(*inputs, *before)


def exchange(blocks, axis):
    return lax.all_to_all(blocks, axis, 0, 0, tiled=True)


def body(
    tokens, lengths, norm_gain, w_z, w_x, w_b, w_c, w_dt, conv_weight, dt_bias, a_log, d_skip, out_gain, w_out,
    conv_state, ssm_state,
):
    tp, dp = lax.axis_size("tp"), lax.axis_size("dp")
    if GROUPS != tp or dp & (dp - 1):
        raise ValueError("unexpected mesh")
    local_heads = HEADS // tp
    rows, features = tokens.shape
    block = rows // dp
    layers = w_z.shape[0]
    w_dt = jnp.swapaxes(w_dt, 1, 2)
    past = jnp.swapaxes(conv_state, 1, 2)
    lengths = lengths.reshape(1, -1)
    across = [2 * k for k in range(1, dp // 2)]

    def over_x(blocks):
        return [blocks[0], *(swapped(b, mask) for b, mask in zip(blocks[1:], across))]

    parts, own_packs = project_first(
        local_heads, block, dp // 2, tokens, norm_gain, w_x, w_b, w_c, w_z, w_dt
    )
    other_packs = [swapped(pack, 1) for pack in own_packs]
    pieces = prepare(parts[0], ssm_state)
    parts = over_x(parts)
    other_out = swapped(w_out, 1)
    streams = [tokens, other_packs[0]]
    made = ()
    for layer in range(layers):
        last = layer == layers - 1
        mixed, *rest = mix(
            layer, parts, lengths, conv_weight, dt_bias, a_log, d_skip, out_gain, past, pieces
        )
        mixed = over_x([mixed] * (dp // 2))
        if layer == 0:
            mixed, other_packs = lax.optimization_barrier((mixed, other_packs))
        if last:
            made = states(layer, PIECES, lengths, past, ssm_state, *rest, made)
            mixed, made = lax.optimization_barrier((mixed, made))
        share = output(layer, mixed, w_out, other_out)
        share = exchange(share.reshape(tp, rows // tp, features), "tp")
        new = exchange(add(block, share, streams), "tp")
        if not last:
            streams = [new.reshape(rows, features)]
            parts = project_later(dp // 2, streams[0], own_packs[layer], other_packs[layer])
            parts, rest = lax.optimization_barrier((parts, rest))
            parts = over_x(parts)
            made = states(layer, PIECES, lengths, past, ssm_state, *rest, made)
            parts, made = lax.optimization_barrier((parts, made))
    conv_new, ssm_new = made
    return order(block, new, swapped(new[tp // 2 :], 1)), jnp.swapaxes(conv_new, 1, 2), ssm_new


def solution(mesh):
    by_seq = ("grp", "dp")
    placed = (
        P("grp", "dp"),
        P(by_seq),
        P(None, "dp"),
        P(None, "dp", "tp"),
        P(None, "dp", "tp"),
        P(None, "dp", "tp"),
        P(None, "dp", "tp"),
        P(None, "dp", None),
        P(None, None, "tp"),
        P(None, "tp"),
        P(None, "tp"),
        P(None, "tp"),
        P(None, "tp"),
        P(None, "tp", "dp"),
        P(None, by_seq, None, "tp"),
        P(None, by_seq, "tp", None, None),
    )
    return jax.shard_map(
        body,
        mesh=mesh,
        in_specs=placed,
        out_specs=(P("grp", "dp"), P(None, by_seq, None, "tp"), P(None, by_seq, "tp", None, None)),
        check_vma=False,
    )
```

```python
import functools

import jax
import jax.numpy as jnp
from jax import lax
from jax.experimental import pallas as pl
from jax.experimental.pallas import tpu as pltpu
from jax.sharding import PartitionSpec as P


D = 4096
HEADS = 64
GROUPS = 16
CONV_W = 4
EPSILON = 1e-06
LANES = 128
PIECE = 16
PIECES = 4
BF16 = jnp.bfloat16
F32 = jnp.float32
MIB = 1 << 20

VMEM_SPEC = pl.BlockSpec(memory_space=pltpu.VMEM)


def params(mib):
    return pltpu.CompilerParams(vmem_limit_bytes=int(mib * MIB))


def iota(shape, dim):
    return lax.broadcasted_iota(jnp.int32, shape, dim)


def dot(a, b, dims):
    return lax.dot_general(a, b, (dims, ((), ())), preferred_element_type=F32)


def as_column(ref):
    count = ref.shape[1]
    same = iota((count, count), 0) == iota((count, count), 1)
    row = jnp.broadcast_to(ref[...].astype(F32), (count, count))
    return jnp.sum(jnp.where(same, row, 0.0), axis=1, keepdims=True)


def split(value):
    high = value.astype(BF16)
    return high, (value - high.astype(F32)).astype(BF16)


def gate_kernel(out_ref):
    out_ref[...] = jnp.zeros_like(out_ref)


def long_cost():
    return pl.CostEstimate(flops=20_000_000_000, bytes_accessed=1_000_000, transcendentals=0)


def gate():
    return pl.pallas_call(
        gate_kernel,
        out_shape=jax.ShapeDtypeStruct((8, LANES), F32),
        out_specs=VMEM_SPEC,
        compiler_params=params(1),
        cost_estimate=long_cost(),
        name="gate",
    )()


def swapped(value, mask):
    pairs = [(i, i ^ mask) for i in range(lax.axis_size("dp"))]
    return lax.ppermute(value, "dp", pairs)


def chosen_heads(heads, local_heads):
    row, column = iota((LANES, heads), 0), iota((LANES, heads), 1)
    local = row % PIECE
    first = lax.axis_index("tp") * local_heads
    return ((column == first + local) & (local < local_heads) & (row < 2 * PIECE)).astype(BF16)


def with_squares(extras, squares):
    return jnp.where(iota(extras.shape, 1) % PIECE == PIECE // 2, squares, extras)


def in_pieces(extras):
    high, low = split(extras)
    return jnp.where(iota(extras.shape, 1) < PIECE, high.astype(F32), low.astype(F32)).astype(BF16)


def block_at(k):
    at = lax.axis_index("dp")
    return lax.bitwise_xor(at // 2, jnp.int32(k)) * 2 + at % 2


def first_rows(local_heads, block, away, x_ref, gain_ref, weights, wdt_ref, out_ref):
    half = x_ref.shape[0] // 2
    blocks = [lax.bitwise_xor(block_at(k), jnp.int32(away)) for k in range(half // block)]
    tokens = [x_ref[pl.ds(pl.multiple_of(b * block, block), block), :] for b in blocks]
    wide = jnp.concatenate(tokens, axis=0).astype(F32)
    normed = (wide * gain_ref[0:1, :]).astype(BF16)
    at = 0
    for ref in weights:
        width = ref.shape[-1]
        out_ref[:, at : at + width] = dot(normed, ref[0], ((1,), (0,))).astype(out_ref.dtype)
        at += width
    chosen = chosen_heads(wdt_ref.shape[1], local_heads)
    steps = dot(wdt_ref[0], chosen, ((0,), (1,))).astype(BF16)
    squares = jnp.sum(wide * wide, axis=-1, keepdims=True)
    extras = with_squares(dot(normed, steps, ((1,), (0,))), squares)
    out_ref[:, at:] = in_pieces(extras) if away else extras


def away_kernel(local_heads, block, x_ref, gain_ref, wx_ref, wb_ref, wc_ref, wz_ref, wdt_ref, _, out_ref):
    first_rows(local_heads, block, 1, x_ref, gain_ref, (wx_ref, wb_ref, wc_ref, wz_ref), wdt_ref, out_ref)


def home_kernel(local_heads, block, x_ref, gain_ref, wx_ref, wb_ref, wc_ref, wz_ref, wdt_ref, own_ref, *packs):
    weights = (wx_ref, wb_ref, wc_ref, wz_ref)
    first_rows(local_heads, block, 0, x_ref, gain_ref, weights, wdt_ref, own_ref)
    features = x_ref.shape[1]
    at = own_ref.shape[1] - LANES
    chosen = chosen_heads(wdt_ref.shape[1], local_heads)
    for layer, pack in enumerate(packs, 1):
        first = 0
        for ref in weights:
            pack[:features, first : first + ref.shape[-1]] = ref[layer]
            first += ref.shape[-1]
        pack[:features, at:] = dot(wdt_ref[layer], chosen, ((0,), (1,))).astype(BF16)
        row = iota((PIECE, features), 0)
        left = jnp.broadcast_to(gain_ref[layer : layer + 1, :], row.shape)
        gains = jnp.zeros_like(left)
        for k in range(3):
            piece = left.astype(BF16).astype(F32)
            gains = jnp.where(row == k, piece, gains)
            left = left - piece
        pack[features : features + PIECE, :features] = gains.astype(BF16)
        pack[features + PIECE :, :features] = x_ref[...]


def combine_kernel(own_ref, arrived_ref, *out_refs):
    total = own_ref[...] + arrived_ref[...].astype(F32)
    at = total.shape[1] - LANES
    pieces = arrived_ref[:, at:].astype(F32)
    whole = pieces + pltpu.roll(pieces, LANES - PIECE, 1)
    whole = jnp.where(iota(whole.shape, 1) < PIECE, whole, pltpu.roll(whole, PIECE, 1))
    tail = in_pieces(own_ref[:, at:] + whole)
    block = total.shape[0] // len(out_refs)
    for k, ref in enumerate(out_refs):
        ref[:, :at] = total[k * block : (k + 1) * block, :at].astype(BF16)
        ref[:, at:] = tail[k * block : (k + 1) * block]


def project_first(local_heads, block, blocks, stream, norm_gain, w_x, w_b, w_c, w_z, w_dt):
    rows, features = stream.shape
    width = sum(w.shape[2] for w in (w_x, w_b, w_c, w_z)) + LANES
    own = jax.ShapeDtypeStruct((rows // 2, width), F32)
    other = jax.ShapeDtypeStruct((rows // 2, width), BF16)
    packs = [jax.ShapeDtypeStruct((features + PIECE + rows, width), BF16)] * (w_z.shape[0] - 1)
    inputs = [stream, norm_gain, w_x, w_b, w_c, w_z, w_dt]
    other = pl.pallas_call(
        functools.partial(away_kernel, local_heads, block),
        out_shape=other,
        in_specs=[VMEM_SPEC] * (1 + len(inputs)),
        out_specs=VMEM_SPEC,
        compiler_params=params(8),
        name="project_away",
    )(*inputs, gate())
    own, *packed = pl.pallas_call(
        functools.partial(home_kernel, local_heads, block),
        out_shape=(own, *packs),
        in_specs=[VMEM_SPEC] * len(inputs),
        out_specs=[VMEM_SPEC] * (1 + len(packs)),
        compiler_params=params(8),
        cost_estimate=pl.CostEstimate(flops=200_000_000, bytes_accessed=2_000_000, transcendentals=0),
        name="project_home",
    )(*inputs)
    arrived = swapped(other, 1)
    parts = pl.pallas_call(
        combine_kernel,
        out_shape=[jax.ShapeDtypeStruct((block, width), BF16)] * blocks,
        in_specs=[VMEM_SPEC] * 2,
        out_specs=[VMEM_SPEC] * blocks,
        compiler_params=params(4),
        cost_estimate=long_cost(),
        name="combine",
    )(own, arrived)
    return parts, packed


def later_kernel(stream_ref, own_ref, other_ref, *out_refs):
    rows, features = stream_ref.shape[0] // 2, stream_ref.shape[1]
    total, squares = 0.0, 0.0
    for k, ref in enumerate((own_ref, other_ref)):
        wide = stream_ref[k * rows : (k + 1) * rows, :].astype(F32)
        pieces = ref[features : features + PIECE, :features].astype(F32)
        gain = pieces[0:1] + pieces[1:2] + pieces[2:3]
        normed = (wide * gain).astype(BF16)
        total = total + dot(normed, ref[:features, :], ((1,), (0,)))
        squares = squares + jnp.sum(wide * wide, axis=-1, keepdims=True)
    at = total.shape[1] - LANES
    tail = in_pieces(with_squares(total[:, at:], squares))
    block = rows // len(out_refs)
    for k, ref in enumerate(out_refs):
        ref[:, :at] = total[k * block : (k + 1) * block, :at].astype(BF16)
        ref[:, at:] = tail[k * block : (k + 1) * block]


def project_later(blocks, stream, own, other):
    rows = stream.shape[0] // 2
    out = jax.ShapeDtypeStruct((rows // blocks, own.shape[1]), BF16)
    return pl.pallas_call(
        later_kernel,
        out_shape=[out] * blocks,
        in_specs=[VMEM_SPEC] * 3,
        out_specs=[VMEM_SPEC] * blocks,
        compiler_params=params(8),
        cost_estimate=long_cost(),
    )(stream, own, other)


def mix_kernel(
    layer, given, *refs
):
    mix_body(layer, refs[:given], *refs[given:])


def mix_body(
    layer, parts, lengths_ref, taps_ref, bias_ref, alog_ref, skip_ref, gain_ref, past_ref, state_ref,
    mixed_ref, scaled_ref, keys_ref, decay_ref, current_ref,
):
    past_ref = past_ref.at[layer]
    seqs = parts[0].shape[0]
    heads = bias_ref.shape[1]
    width_x, width_n = state_ref.shape[2], state_ref.shape[3]
    head_dim = width_x // heads
    conv = width_x + 2 * width_n
    total = sum(part[...].astype(F32) for part in parts)
    extras = total[:, conv + width_x :]
    extras = extras + pltpu.roll(extras, LANES - PIECE, 1)
    inverse = lax.rsqrt(extras[:, PIECE // 2 : PIECE // 2 + 1] / D + EPSILON)
    current = (total[:, :conv] * inverse).astype(BF16)
    gating = (total[:, conv : conv + width_x] * inverse).astype(BF16).astype(F32)
    current_ref[...] = current

    row = iota((seqs, 1), 0)
    lengths = as_column(lengths_ref)
    taps = taps_ref[layer].astype(F32)
    summed = current.astype(F32) * taps[CONV_W - 1 : CONV_W]
    for j in range(CONV_W - 1):
        past = past_ref[j].astype(F32)
        summed = summed + jnp.where(lengths + j >= CONV_W, past, 0.0) * taps[j : j + 1]
    activated = summed / (1.0 + jnp.exp(-summed))
    head_in = activated[:, :width_x]
    write_keys = activated[:, width_x : width_x + width_n]
    read_keys = activated[:, width_x + width_n :]

    raw = extras[:, :heads] * inverse + bias_ref[layer : layer + 1, :]
    step = jnp.maximum(raw, 0.0) + jnp.log1p(jnp.exp(-jnp.abs(raw)))
    decay = jnp.exp(-jnp.exp(alog_ref[layer : layer + 1, :]) * step)
    decay = jnp.where(lengths >= 2, decay, 0.0)
    lane = iota((seqs, width_x), 1)

    def spread(value):
        out = value[:, 0:1]
        for h in range(1, heads):
            out = jnp.where(lane >= h * head_dim, value[:, h : h + 1], out)
        return out

    scaled = spread(step) * head_in
    scaled_ref[...] = scaled
    keys_ref[...] = write_keys
    decay_ref[...] = decay

    left = jnp.concatenate(split(read_keys), axis=0)
    seen = jnp.zeros((seqs, width_x), F32)
    for s in range(seqs):
        both = dot(left, state_ref[layer, s], ((1,), (1,)))
        seen = jnp.where(row == s, both[:seqs] + both[seqs:], seen)
    pair = jnp.sum(write_keys * read_keys, axis=-1, keepdims=True)
    readout = spread(decay) * seen + scaled * pair + spread(skip_ref[layer : layer + 1, :]) * head_in
    gated = readout * (gating / (1.0 + jnp.exp(-gating)))
    mean = jnp.mean(gated * gated, axis=-1, keepdims=True)
    mixed = (gated * lax.rsqrt(mean + EPSILON) * gain_ref[layer : layer + 1, :]).astype(BF16)
    mixed_ref[...] = mixed


def mix(layer, parts, lengths, taps, bias, alog, skip, gain, past, state):
    seqs = parts[0].shape[-2]
    heads, width_x, width_n = bias.shape[1], state.shape[2], state.shape[3]
    shapes = (
        jax.ShapeDtypeStruct((seqs, width_x), BF16),
        jax.ShapeDtypeStruct((seqs, width_x), F32),
        jax.ShapeDtypeStruct((seqs, width_n), F32),
        jax.ShapeDtypeStruct((seqs, heads), F32),
        jax.ShapeDtypeStruct((seqs, width_x + 2 * width_n), BF16),
    )
    return pl.pallas_call(
        functools.partial(mix_kernel, layer, len(parts)),
        out_shape=shapes,
        in_specs=[*[VMEM_SPEC] * (len(parts) + 8)],
        out_specs=[VMEM_SPEC] * len(shapes),
        compiler_params=params(12),
    )(*parts, lengths, taps, bias, alog, skip, gain, past, state)


def output_kernel(layer, given, *refs):
    mixed = jnp.concatenate([ref[...] for ref in refs[:given]], axis=0)
    own_ref, other_ref, out_ref = refs[given:]
    rows = mixed.shape[0]
    for k, ref in enumerate((own_ref, other_ref)):
        out_ref[k * rows : (k + 1) * rows, :] = dot(mixed, ref[layer], ((1,), (0,))).astype(BF16)


def output(layer, mixed, own, other):
    rows = sum(m.shape[0] for m in mixed)
    return pl.pallas_call(
        functools.partial(output_kernel, layer, len(mixed)),
        out_shape=jax.ShapeDtypeStruct((2 * rows, own.shape[2]), BF16),
        in_specs=[VMEM_SPEC] * (len(mixed) + 2),
        out_specs=VMEM_SPEC,
        compiler_params=params(4),
    )(*mixed, own, other)


def add_kernel(block, parts_ref, *refs):
    streams, out_ref = refs[:-1], refs[-1]
    copies, rows, _ = parts_ref.shape
    total = sum(parts_ref[k].astype(F32) for k in range(copies))
    at = lax.axis_index("tp")
    if len(streams) == 1:
        old = streams[0][pl.ds(pl.multiple_of(at * rows, rows), rows), :]
    else:
        half = copies // 2
        group = lax.rem(at, half)
        per = block // rows
        start = block_at(group // per) * block + lax.rem(group, per) * rows
        first, second = streams
        features = out_ref.shape[-1]
        lowest = second.shape[0] - first.shape[0]
        picked = [
            first[pl.ds(pl.multiple_of(start, rows), rows), :],
            second[pl.ds(pl.multiple_of(lowest + start, rows), rows), :features],
        ]
        old = jnp.where(at < half, picked[0], picked[1])
    new = (old.astype(F32) + total).astype(BF16)
    for k in range(copies):
        out_ref[k] = new


def add(block, parts, streams):
    return pl.pallas_call(
        functools.partial(add_kernel, block),
        out_shape=jax.ShapeDtypeStruct(parts.shape, BF16),
        in_specs=[VMEM_SPEC] * (1 + len(streams)),
        out_specs=VMEM_SPEC,
        compiler_params=params(4),
    )(parts, *streams)


def order_kernel(block, own_ref, other_ref, out_ref):
    copies, rows, _ = own_ref.shape
    per = block // rows
    half = copies // 2
    for k in range(half // per):
        index = block_at(k)
        for ref, at in ((own_ref, index), (other_ref, lax.bitwise_xor(index, jnp.int32(1)))):
            value = jnp.concatenate([ref[k * per + s] for s in range(per)], axis=0)
            out_ref[pl.ds(pl.multiple_of(at * block, block), block), :] = value


def order(block, own, other):
    copies, rows, features = own.shape
    return pl.pallas_call(
        functools.partial(order_kernel, block),
        out_shape=jax.ShapeDtypeStruct((copies * rows, features), BF16),
        in_specs=[VMEM_SPEC] * 2,
        out_specs=VMEM_SPEC,
        compiler_params=params(4),
        name="order",
    )(own, other)


def prepare_kernel(_, state_ref, out_ref):
    layers, seqs, heads, head_dim, width_n = state_ref.shape
    for layer in range(layers):
        for s in range(seqs):
            out_ref[layer, s] = state_ref[layer, s].reshape(heads * head_dim, width_n).astype(BF16)


def prepare(after, state):
    layers, seqs, heads, head_dim, width_n = state.shape
    return pl.pallas_call(
        prepare_kernel,
        out_shape=jax.ShapeDtypeStruct((layers, seqs, heads * head_dim, width_n), BF16),
        in_specs=[VMEM_SPEC] * 2,
        out_specs=VMEM_SPEC,
        compiler_params=params(12),
        cost_estimate=pl.CostEstimate(flops=500_000_000, bytes_accessed=2 * state.size, transcendentals=0),
        name="prepare",
    )(after, state)


def states_kernel(layer, pieces, lengths_ref, past_ref, state_ref, scaled_ref, keys_ref, decay_ref, current_ref, *refs):
    conv_ref, new_ref, columns, conv, new, left = refs[-6:]
    seqs, heads, head_dim, _ = new.shape
    piece = seqs // pieces

    def copy(k):
        rows = pl.ds(k * piece, piece)
        return pltpu.make_async_copy(new.at[rows], new_ref.at[layer, rows], left.at[k])

    scaled = scaled_ref[...]
    rest = jnp.zeros((LANES - seqs, scaled.shape[1]), F32)
    columns[...] = jnp.concatenate([scaled, rest], axis=0).T
    for s in range(seqs):
        for h in range(heads):
            column = columns[h * head_dim : (h + 1) * head_dim, s : s + 1]
            old = decay_ref[s : s + 1, h : h + 1] * state_ref[layer, s, h]
            new[s, h] = old + column * keys_ref[s : s + 1, :]
        if s % piece == 0 and s > 0:
            copy(s // piece - 1).start()
    lengths = as_column(lengths_ref)
    for j in range(1, CONV_W - 1):
        past = past_ref[layer, j].astype(F32)
        conv[j - 1] = jnp.where(lengths + j >= CONV_W, past, 0.0).astype(BF16)
    conv[CONV_W - 2] = current_ref[...]
    copy(pieces - 1).start()
    for k in range(pieces):
        copy(k).wait()
    last = pltpu.make_async_copy(conv, conv_ref.at[layer], left.at[pieces])
    last.start()
    last.wait()


def states(layer, pieces, lengths, past, state, scaled, keys, decay, current, before):
    _, heads, head_dim, _ = state.shape[1:]
    anywhere = pl.BlockSpec(memory_space=pl.ANY)
    inputs = (lengths, past, state, scaled, keys, decay, current)
    return pl.pallas_call(
        functools.partial(states_kernel, layer, pieces),
        out_shape=(jax.ShapeDtypeStruct(past.shape, past.dtype), jax.ShapeDtypeStruct(state.shape, F32)),
        in_specs=[*[VMEM_SPEC] * len(inputs), *[anywhere] * len(before)],
        out_specs=(anywhere, anywhere),
        input_output_aliases={len(inputs) + k: k for k in range(len(before))},
        scratch_shapes=[
            pltpu.VMEM((heads * head_dim, LANES), F32),
            pltpu.VMEM(past.shape[1:], BF16),
            pltpu.VMEM(state.shape[1:], F32),
            pltpu.SemaphoreType.DMA((pieces + 1,)),
        ],
        compiler_params=params(8),
        cost_estimate=pl.CostEstimate(flops=2_000_000_000, bytes_accessed=4 * state.size, transcendentals=0),
    )(*inputs, *before)


def exchange(blocks, axis):
    return lax.all_to_all(blocks, axis, 0, 0, tiled=True)


def body(
    tokens, lengths, norm_gain, w_z, w_x, w_b, w_c, w_dt, conv_weight, dt_bias, a_log, d_skip, out_gain, w_out,
    conv_state, ssm_state,
):
    tp, dp = lax.axis_size("tp"), lax.axis_size("dp")
    if GROUPS != tp or dp & (dp - 1):
        raise ValueError("unexpected mesh")
    local_heads = HEADS // tp
    rows, features = tokens.shape
    block = rows // dp
    layers = w_z.shape[0]
    w_dt = jnp.swapaxes(w_dt, 1, 2)
    past = jnp.swapaxes(conv_state, 1, 2)
    lengths = lengths.reshape(1, -1)
    across = [2 * k for k in range(1, dp // 2)]

    def over_x(blocks):
        return [blocks[0], *(swapped(b, mask) for b, mask in zip(blocks[1:], across))]

    parts, own_packs = project_first(
        local_heads, block, dp // 2, tokens, norm_gain, w_x, w_b, w_c, w_z, w_dt
    )
    other_packs = [swapped(pack, 1) for pack in own_packs]
    pieces = prepare(parts[0], ssm_state)
    parts = over_x(parts)
    other_out = swapped(w_out, 1)
    streams = [tokens, other_packs[0]]
    made = ()
    for layer in range(layers):
        last = layer == layers - 1
        mixed, *rest = mix(
            layer, parts, lengths, conv_weight, dt_bias, a_log, d_skip, out_gain, past, pieces
        )
        mixed = over_x([mixed] * (dp // 2))
        if layer == 0:
            mixed, other_packs = lax.optimization_barrier((mixed, other_packs))
        if last:
            made = states(layer, PIECES, lengths, past, ssm_state, *rest, made)
            mixed, made = lax.optimization_barrier((mixed, made))
        share = output(layer, mixed, w_out, other_out)
        share = exchange(share.reshape(tp, rows // tp, features), "tp")
        new = exchange(add(block, share, streams), "tp")
        if not last:
            streams = [new.reshape(rows, features)]
            parts = project_later(dp // 2, streams[0], own_packs[layer], other_packs[layer])
            parts, rest = lax.optimization_barrier((parts, rest))
            parts = over_x(parts)
            made = states(layer, PIECES, lengths, past, ssm_state, *rest, made)
            parts, made = lax.optimization_barrier((parts, made))
    conv_new, ssm_new = made
    return order(block, new, swapped(new[tp // 2 :], 1)), jnp.swapaxes(conv_new, 1, 2), ssm_new


def solution(mesh):
    by_seq = ("grp", "dp")
    placed = (
        P("grp", "dp"),
        P(by_seq),
        P(None, "dp"),
        P(None, "dp", "tp"),
        P(None, "dp", "tp"),
        P(None, "dp", "tp"),
        P(None, "dp", "tp"),
        P(None, "dp", None),
        P(None, None, "tp"),
        P(None, "tp"),
        P(None, "tp"),
        P(None, "tp"),
        P(None, "tp"),
        P(None, "tp", "dp"),
        P(None, by_seq, None, "tp"),
        P(None, by_seq, "tp", None, None),
    )
    return jax.shard_map(
        body,
        mesh=mesh,
        in_specs=placed,
        out_specs=(P("grp", "dp"), P(None, by_seq, None, "tp"), P(None, by_seq, "tp", None, None)),
        check_vma=False,
    )
```
